768 devices in a mesh: fs: 48 (over z, x), tp: 16 (over y, core).
Axes of the slice: x: 4, y: 8, z: 12, core: 2. Of those that a mesh axis runs over, the one named last changes fastest.
Arguments:
- tokens: bfloat16 [21504, 2304], P('fs'), may hold values from -6 to 6
- norm_gain: float32 [2304], replicated, may hold values from 0.1 to 1.9
- gate_weight: bfloat16 [2304, 6144], P('fs', 'tp'), may hold values from -0.125 to 0.125
- up_weight: bfloat16 [2304, 6144], P('fs', 'tp'), may hold values from -0.125 to 0.125
- down_weight: bfloat16 [6144, 2304], P('tp', 'fs'), may hold values from -0.078125 to 0.078125
- branch_gain: float32 [2304], replicated, may hold values from 0.1 to 1.9
Outputs:
- result: bfloat16 [21504, 2304], P('fs')
The draws below stay inside these ranges and needn't reach their ends.
All inputs are finite; a program needn't handle non-finite values.
Results may differ from the reference program's by a relative error of at most 0.014.
Values may be sent and summed in bfloat16 or wider, within the bound.
No kernel may reach another device: no remote copies, remote signals or barrier semaphores. Data moves between devices by JAX's collectives and lax.ppermute only.
A program may use at most 32 MiB of HBM per device.

```python
import jax
import jax.numpy as jnp
from jax import lax

D = 2304
FF = 6144
TOKENS = 21504
N_TP = 16


def shard_levels(own_key, dims, split, smallest, high):
    level, own = 1.0, jax.random.fold_in(own_key, 6)
    for position, blocks in split:
        draws = jnp.exp(jax.random.uniform(jax.random.fold_in(own, position), (blocks,), jnp.float32, smallest / len(split), high / len(split)))
        level = level * jnp.repeat(draws, dims[position] // blocks).reshape([-1 if axis == position else 1 for axis in range(len(dims))])
    return level


def scatter_about(rng, shape, spread, bound, split=(), held_as=jnp.bfloat16):
    entries = jax.random.normal(rng, shape, jnp.float32) * spread
    if len(split) > 0:
        entries = shard_levels(rng, shape, split, -0.22, 0.18) * entries
    return jnp.clip(entries, min=-bound, max=bound).astype(held_as)


def setup_inputs(seed: int = 0) -> dict:
    key_of = jax.random.split(jax.random.key(seed), 7)
    tokens = scatter_about(key_of[0], (TOKENS, D), 1.0, 6.0, ((0, 48),))
    norm_gain = jnp.clip(1.0 + 0.18 * jax.random.normal(key_of[1], (D,), jnp.float32), 0.1, 1.9)
    gate_weight = scatter_about(key_of[2], (D, FF), D ** -0.5, 0.125, ((0, 48), (1, 16)))
    up_weight = scatter_about(key_of[3], (D, FF), D ** -0.5, 0.125, ((0, 48), (1, 16)))
    down_weight = scatter_about(key_of[4], (FF, D), FF ** -0.5, 0.078125, ((0, 16), (1, 48)))
    branch_gain = jnp.clip(1.0 + 0.18 * jax.random.normal(key_of[5], (D,), jnp.float32), 0.1, 1.9)
    return {"tokens": tokens, "norm_gain": norm_gain, "gate_weight": gate_weight, "up_weight": up_weight, "down_weight": down_weight, "branch_gain": branch_gain}


epsilon = 1e-06

def reference(tokens, norm_gain, gate_weight, up_weight, down_weight, branch_gain):
    widened = tokens.astype(jnp.float32)
    scale = lax.rsqrt(lax.optimization_barrier(jnp.mean(widened * widened, axis=-1, keepdims=True)) + epsilon)
    normed = (widened * scale * norm_gain).astype(jnp.bfloat16)
    width = FF // N_TP
    branch = jnp.zeros(tokens.shape, jnp.float32)
    for block_index in range(N_TP):
        begin = block_index * width
        gate_sum = jnp.dot(normed, gate_weight[:, begin:begin + width], preferred_element_type=jnp.float32)
        up_sum = jnp.dot(normed, up_weight[:, begin:begin + width], preferred_element_type=jnp.float32)
        hidden = (jax.nn.silu(gate_sum) * up_sum).astype(jnp.bfloat16)
        partial_value = jnp.dot(hidden, down_weight[begin:begin + width, :], preferred_element_type=jnp.float32)
        branch = branch + partial_value.astype(jnp.bfloat16).astype(jnp.float32)
    branch_scale = lax.rsqrt(lax.optimization_barrier(jnp.mean(branch * branch, axis=-1, keepdims=True)) + epsilon)
    return (widened + branch * branch_scale * branch_gain).astype(jnp.bfloat16)
```

```python
import jax
import jax.numpy as jnp
from jax import lax
from jax.experimental import pallas as pl
from jax.experimental.pallas import tpu as pltpu
from jax.sharding import Mesh
from jax.sharding import PartitionSpec as P


epsilon = 1e-06
VMEM = pltpu.VMEM
BF16 = jnp.bfloat16
F32 = jnp.float32


def shift(value, axis, by):
    n = lax.axis_size(axis)
    return lax.ppermute(value, axis, [(i, (i + by) % n) for i in range(n)])


def after(value, *others):
    return lax.optimization_barrier((value, *others))[0]


def local_call(body, outs, scratch=(), n_scalars=0, n_in=0):
    return pl.pallas_call(
        body,
        out_shape=outs,
        in_specs=[pl.BlockSpec(memory_space=pltpu.SMEM)] * n_scalars
        + [pl.BlockSpec(memory_space=VMEM)] * n_in,
        out_specs=jax.tree.map(lambda _: pl.BlockSpec(memory_space=VMEM), outs),
        scratch_shapes=list(scratch),
        compiler_params=pltpu.CompilerParams(vmem_limit_bytes=48 << 20),
    )


def across_x(block):
    half = block.shape[0] // 2
    left, right = shift(block, "x", 1), shift(block, "x", -1)
    return left, right, shift(left[:half], "x", 1), shift(right[half:], "x", -1)


def assemble(x, pieces, whole):
    own, left, right, low, high = pieces
    slots = [lax.rem(x + k, 4) for k in range(4)]
    planes = own.shape[0]
    for z in range(planes):
        whole[z, slots[0]] = own[z]
        whole[z, slots[1]] = right[z]
        whole[z, slots[3]] = left[z]
        whole[z, slots[2]] = low[z] if z < planes // 2 else high[z - planes // 2]


def hidden_body(x_ref, normed, own, left, right, low, high, hidden, whole):
    assemble(x_ref[0], (own, left, right, low, high), whole)
    planes, across, rows, columns = whole.shape
    weight = whole[...].reshape(planes * across * rows, columns)
    width = columns // 2
    both = jnp.dot(normed[...], weight, preferred_element_type=F32)
    gate, up = both[:, :width], both[:, width:]
    hidden[...] = (gate * jax.nn.sigmoid(gate) * up).astype(BF16)


def partial_body(x_ref, c_ref, hidden, own, left, right, low, high, keep, send, whole):
    assemble(x_ref[0], (own, left, right, low, high), whole)
    planes, across, rows, width = whole.shape
    weight = whole[...].reshape(planes * across * rows, width)
    half = hidden.shape[0] // 2
    for out, which in ((keep, c_ref[0]), (send, 1 - c_ref[0])):
        lines = hidden[pl.ds(pl.multiple_of(which * half, 32), half), :]
        out[...] = lax.dot_general(
            lines, weight, (((1,), (1,)), ((), ())), preferred_element_type=F32
        ).astype(BF16)


def pair_sum_body(mine, theirs, out, total):
    total[...] = mine[...].astype(F32) + theirs[...].astype(F32)
    count, rows, _ = out.shape
    for j in range(count):
        out[j] = total[j * rows : (j + 1) * rows, :].astype(BF16)


def finish_body(pieces, tokens, gain, out):
    branch = pieces[0].astype(F32)
    for j in range(1, pieces.shape[0]):
        branch = branch + pieces[j].astype(F32)
    scale = lax.rsqrt(jnp.mean(branch * branch, axis=-1, keepdims=True) + epsilon)
    out[...] = (tokens[...].astype(F32) + branch * scale * gain[...]).astype(BF16)


def join_body(c_ref, mine, theirs, out, lines):
    count, rows, _ = mine.shape
    half = count * rows
    for source, which in ((mine, c_ref[0]), (theirs, 1 - c_ref[0])):
        for j in range(count):
            lines[j * rows : (j + 1) * rows, :] = source[j].astype(F32)
        out[pl.ds(pl.multiple_of(which * half, 32), half), :] = lines[...].astype(BF16)


def per_device(tokens, norm_gain, gate_weight, up_weight, down_weight, branch_gain):
    x, y, c = (lax.axis_index(a) for a in ("x", "y", "c"))
    x1, c1 = x.astype(jnp.int32)[None], c.astype(jnp.int32)[None]
    n_x, n_y = lax.axis_size("x"), lax.axis_size("y")
    count, width = tokens.shape
    half, rows = count // 2, count // 2 // n_y
    units = gate_weight.shape[1]

    both = jnp.concatenate([gate_weight, up_weight], axis=1)
    both_z = lax.all_gather(both, "z")
    both_x = across_x(both_z)
    down_z = lax.all_gather(after(down_weight.T, both_z), "z")
    down_x = across_x(after(down_z, both_x[0], both_x[1]))

    widened = tokens.astype(F32)
    scale = lax.rsqrt(jnp.mean(widened * widened, axis=-1, keepdims=True) + epsilon)
    normed = (widened * scale * norm_gain).astype(BF16)
    n_z, piece = both_z.shape[0], both_z.shape[1]
    hidden = local_call(
        hidden_body,
        jax.ShapeDtypeStruct((count, units), BF16),
        [VMEM((n_z, n_x, piece, 2 * units), BF16)],
        1, 6,
    )(x1, normed, both_z, *both_x)
    keep, send = local_call(
        partial_body,
        [jax.ShapeDtypeStruct((half, width), BF16)] * 2,
        [VMEM((n_z, n_x, piece, units), BF16)],
        2, 6,
    )(x1, c1, hidden, down_z, *down_x)
    pair = local_call(
        pair_sum_body,
        jax.ShapeDtypeStruct((n_y, rows, width), BF16),
        [VMEM((half, width), F32)],
        0, 2,
    )(keep, shift(send, "c", 1))
    pieces = lax.all_to_all(pair, "y", 0, 0, tiled=True)
    own_tokens = lax.dynamic_slice_in_dim(tokens, c * half + y * rows, rows, 0)
    done = local_call(
        finish_body, jax.ShapeDtypeStruct((rows, width), BF16), (), 0, 3
    )(pieces, own_tokens, branch_gain[None])
    mine = lax.all_gather(done, "y")
    return local_call(
        join_body,
        jax.ShapeDtypeStruct((count, width), BF16),
        [VMEM((half, width), F32)],
        1, 2,
    )(c1, mine, shift(mine, "c", 1))


def solution(mesh):
    n_tp = mesh.shape["tp"]
    split = Mesh(mesh.devices.reshape(12, 4, n_tp // 2, 2), ("z", "x", "y", "c"))
    fs, tp = ("z", "x"), ("y", "c")
    placed = (P(fs, None), P(), P(fs, tp), P(fs, tp), P(tp, fs), P())
    return jax.shard_map(
        per_device, mesh=split, in_specs=placed, out_specs=P(fs, None), check_vma=False
    )
```

```python
import jax
import jax.numpy as jnp
from jax import lax
from jax.experimental import pallas as pl
from jax.experimental.pallas import tpu as pltpu
from jax.sharding import Mesh
from jax.sharding import PartitionSpec as P


epsilon = 1e-06
VMEM = pltpu.VMEM
BF16 = jnp.bfloat16
F32 = jnp.float32


def shift(value, axis, by):
    n = lax.axis_size(axis)
    return lax.ppermute(value, axis, [(i, (i + by) % n) for i in range(n)])


def after(value, *others):
    return lax.optimization_barrier((value, *others))[0]


def local_call(body, outs, scratch=(), n_scalars=0, n_in=0):
    return pl.pallas_call(
        body,
        out_shape=outs,
        in_specs=[pl.BlockSpec(memory_space=pltpu.SMEM)] * n_scalars
        + [pl.BlockSpec(memory_space=VMEM)] * n_in,
        out_specs=jax.tree.map(lambda _: pl.BlockSpec(memory_space=VMEM), outs),
        scratch_shapes=list(scratch),
        compiler_params=pltpu.CompilerParams(vmem_limit_bytes=48 << 20),
    )


def across_x(block):
    copies = jnp.broadcast_to(block[None], (lax.axis_size("x"), *block.shape))
    return lax.all_to_all(copies, "x", 0, 0, tiled=True)


def interleave(blocks, whole):
    for z in range(blocks.shape[1]):
        for x in range(blocks.shape[0]):
            whole[z, x] = blocks[x, z]


def hidden_body(normed, blocks, hidden, whole):
    interleave(blocks, whole)
    planes, across, rows, columns = whole.shape
    weight = whole[...].reshape(planes * across * rows, columns)
    width = columns // 2
    both = jnp.dot(normed[...], weight, preferred_element_type=F32)
    gate, up = both[:, :width], both[:, width:]
    hidden[...] = (gate * jax.nn.sigmoid(gate) * up).astype(BF16)


def half_product(hidden, which, weight):
    half = hidden.shape[0] // 2
    lines = hidden[pl.ds(pl.multiple_of(which * half, 32), half), :]
    planes, across, rows, width = weight.shape
    return lax.dot_general(
        lines,
        weight[...].reshape(planes * across * rows, width),
        (((1,), (1,)), ((), ())),
        preferred_element_type=F32,
    ).astype(BF16)


def send_body(c_ref, hidden, blocks, send, whole):
    interleave(blocks, whole)
    send[...] = half_product(hidden, 1 - c_ref[0], whole)


def keep_body(c_ref, hidden, whole, keep):
    keep[...] = half_product(hidden, c_ref[0], whole)


def pair_sum_body(mine, theirs, out, total, folded):
    total[...] = mine[...].astype(F32) + theirs[...].astype(F32)
    count, rows, width = out.shape
    rows = rows // 2
    for j in range(count):
        for part in range(2):
            folded[j, part * rows : (part + 1) * rows, :] = total[
                j * rows : (j + 1) * rows, part * width : (part + 1) * width
            ]
        out[j] = folded[j].astype(BF16)


def finish_body(pieces, tokens, gain, out, branch, full):
    total = pieces[0].astype(F32)
    for j in range(1, pieces.shape[0]):
        total = total + pieces[j].astype(F32)
    branch[...] = total
    rows, width = tokens.shape[0], total.shape[1]
    parts = [branch[part * rows : (part + 1) * rows, :] for part in range(2)]
    squares = sum(jnp.sum(p * p, axis=-1, keepdims=True) for p in parts)
    scale = lax.rsqrt(squares / (2 * width) + epsilon)
    for part, value in enumerate(parts):
        columns = slice(part * width, (part + 1) * width)
        full[part * rows : (part + 1) * rows, :] = (
            tokens[:, columns].astype(F32) + value * scale * gain[:, columns]
        )
    out[...] = full[...].astype(BF16)


def join_body(c_ref, mine, theirs, out, folded, lines):
    count, rows, width = mine.shape
    rows = rows // 2
    half = count * rows
    for at, (source, which) in enumerate(((mine, c_ref[0]), (theirs, 1 - c_ref[0]))):
        for j in range(count):
            folded[at, j] = source[j].astype(F32)
            for part in range(2):
                lines[at, j * rows : (j + 1) * rows, part * width : (part + 1) * width] = (
                    folded[at, j, part * rows : (part + 1) * rows, :]
                )
        out[pl.ds(pl.multiple_of(which * half, 32), half), :] = lines[at].astype(BF16)


def per_device(tokens, norm_gain, gate_weight, up_weight, down_weight, branch_gain):
    y, c = lax.axis_index("y"), lax.axis_index("c")
    c1 = c.astype(jnp.int32)[None]
    n_x, n_y, n_z = (lax.axis_size(a) for a in ("x", "y", "z"))
    count, width = tokens.shape
    half, rows = count // 2, count // 2 // n_y
    units, piece = gate_weight.shape[1], gate_weight.shape[0]
    folded = (n_y, 2 * rows, width // 2)

    both_z = lax.all_gather(jnp.concatenate([gate_weight, up_weight], axis=1), "z")
    both = across_x(both_z)
    down = across_x(lax.all_gather(after(down_weight.T, both_z), "z"))

    widened = tokens.astype(F32)
    scale = lax.rsqrt(jnp.mean(widened * widened, axis=-1, keepdims=True) + epsilon)
    normed = (widened * scale * norm_gain).astype(BF16)
    hidden = local_call(
        hidden_body,
        jax.ShapeDtypeStruct((count, units), BF16),
        [VMEM((n_z, n_x, piece, 2 * units), BF16)],
        0, 2,
    )(normed, both)
    send, whole = local_call(
        send_body,
        [
            jax.ShapeDtypeStruct((half, width), BF16),
            jax.ShapeDtypeStruct((n_z, n_x, piece, units), BF16),
        ],
        (), 1, 2,
    )(c1, hidden, down)
    theirs = shift(send, "c", 1)
    keep = local_call(
        keep_body, jax.ShapeDtypeStruct((half, width), BF16), (), 1, 2
    )(c1, hidden, whole)
    pair = local_call(
        pair_sum_body,
        jax.ShapeDtypeStruct(folded, BF16),
        [VMEM((half, width), F32), VMEM(folded, F32)],
        0, 2,
    )(keep, theirs)
    pieces = lax.all_to_all(pair, "y", 0, 0, tiled=True)
    own_tokens = lax.dynamic_slice_in_dim(tokens, c * half + y * rows, rows, 0)
    done = local_call(
        finish_body,
        jax.ShapeDtypeStruct(folded[1:], BF16),
        [VMEM(folded[1:], F32)] * 2,
        0, 3,
    )(pieces, own_tokens, branch_gain[None])
    mine = lax.all_gather(done, "y")
    return local_call(
        join_body,
        jax.ShapeDtypeStruct((count, width), BF16),
        [VMEM((2, *folded), F32), VMEM((2, half, width), F32)],
        1, 2,
    )(c1, mine, shift(mine, "c", 1))


def solution(mesh):
    n_tp = mesh.shape["tp"]
    split = Mesh(mesh.devices.reshape(12, 4, n_tp // 2, 2), ("z", "x", "y", "c"))
    fs, tp = ("z", "x"), ("y", "c")
    placed = (P(fs, None), P(), P(fs, tp), P(fs, tp), P(tp, fs), P())
    return jax.shard_map(
        per_device, mesh=split, in_specs=placed, out_specs=P(fs, None), check_vma=False
    )
```

```python
import jax
import jax.numpy as jnp
from jax import lax
from jax.experimental import pallas as pl
from jax.experimental.pallas import tpu as pltpu
from jax.sharding import Mesh
from jax.sharding import PartitionSpec as P


epsilon = 1e-06
VMEM = pltpu.VMEM
BF16 = jnp.bfloat16
F32 = jnp.float32


def shift(value, axis, by):
    n = lax.axis_size(axis)
    return lax.ppermute(value, axis, [(i, (i + by) % n) for i in range(n)])


def after(value, *others):
    return lax.optimization_barrier((value, *others))[0]


def local_call(body, outs, scratch=(), n_scalars=0, n_in=0):
    return pl.pallas_call(
        body,
        out_shape=outs,
        in_specs=[pl.BlockSpec(memory_space=pltpu.SMEM)] * n_scalars
        + [pl.BlockSpec(memory_space=VMEM)] * n_in,
        out_specs=jax.tree.map(lambda _: pl.BlockSpec(memory_space=VMEM), outs),
        scratch_shapes=list(scratch),
        compiler_params=pltpu.CompilerParams(vmem_limit_bytes=48 << 20),
    )


def copies_for(block, axis):
    return jnp.broadcast_to(block[None], (lax.axis_size(axis), *block.shape))


def across_x(block):
    return block, shift(block, "x", -1), shift(block, "x", 1), shift(block, "x", 2)


def interleave(x, blocks, whole):
    for block, offset in zip(blocks, (0, 1, 3, 2), strict=True):
        at = lax.rem(x + offset, 4)
        for z in range(block.shape[0]):
            whole[z, at] = block[z]


def hidden_body(x_ref, normed, own, right, left, far, hidden, whole):
    interleave(x_ref[0], (own, right, left, far), whole)
    planes, across, rows, columns = whole.shape
    weight = whole[...].reshape(planes * across * rows, columns)
    width = columns // 2
    both = jnp.dot(normed[...], weight, preferred_element_type=F32)
    gate, up = both[:, :width], both[:, width:]
    hidden[...] = (gate * jax.nn.sigmoid(gate) * up).astype(BF16)


def half_product(hidden, which, weight):
    half = hidden.shape[0] // 2
    lines = hidden[pl.ds(pl.multiple_of(which * half, 32), half), :]
    planes, across, rows, width = weight.shape
    return lax.dot_general(
        lines,
        weight[...].reshape(planes * across * rows, width),
        (((1,), (1,)), ((), ())),
        preferred_element_type=F32,
    ).astype(BF16)


def send_body(x_ref, c_ref, hidden, own, right, left, far, send, whole):
    interleave(x_ref[0], (own, right, left, far), whole)
    send[...] = half_product(hidden, 1 - c_ref[0], whole)


def keep_body(c_ref, hidden, whole, keep):
    keep[...] = half_product(hidden, c_ref[0], whole)


def pair_sum_body(mine, theirs, out, total, folded):
    total[...] = mine[...].astype(F32) + theirs[...].astype(F32)
    count, rows, width = out.shape
    rows = rows // 2
    for j in range(count):
        for part in range(2):
            folded[j, part * rows : (part + 1) * rows, :] = total[
                j * rows : (j + 1) * rows, part * width : (part + 1) * width
            ]
        out[j] = folded[j].astype(BF16)


def finish_body(pieces, tokens, gain, out, branch, full):
    total = pieces[0].astype(F32)
    for j in range(1, pieces.shape[0]):
        total = total + pieces[j].astype(F32)
    branch[...] = total
    rows, width = tokens.shape[0], total.shape[1]
    parts = [branch[part * rows : (part + 1) * rows, :] for part in range(2)]
    squares = sum(jnp.sum(p * p, axis=-1, keepdims=True) for p in parts)
    scale = lax.rsqrt(squares / (2 * width) + epsilon)
    for part, value in enumerate(parts):
        columns = slice(part * width, (part + 1) * width)
        full[part * rows : (part + 1) * rows, :] = (
            tokens[:, columns].astype(F32) + value * scale * gain[:, columns]
        )
    out[...] = full[...].astype(BF16)


def join_body(c_ref, mine, theirs, out, folded, lines):
    count, rows, width = mine.shape
    rows = rows // 2
    half = count * rows
    for at, (source, which) in enumerate(((mine, c_ref[0]), (theirs, 1 - c_ref[0]))):
        for j in range(count):
            folded[at, j] = source[j].astype(F32)
            for part in range(2):
                lines[at, j * rows : (j + 1) * rows, part * width : (part + 1) * width] = (
                    folded[at, j, part * rows : (part + 1) * rows, :]
                )
        out[pl.ds(pl.multiple_of(which * half, 32), half), :] = lines[at].astype(BF16)


def per_device(tokens, norm_gain, gate_weight, up_weight, down_weight, branch_gain):
    x, y, c = (lax.axis_index(a) for a in ("x", "y", "c"))
    x1, c1 = x.astype(jnp.int32)[None], c.astype(jnp.int32)[None]
    n_x, n_y, n_z = (lax.axis_size(a) for a in ("x", "y", "z"))
    count, width = tokens.shape
    half, rows = count // 2, count // 2 // n_y
    units, piece = gate_weight.shape[1], gate_weight.shape[0]
    folded = (n_y, 2 * rows, width // 2)

    both_z = lax.all_gather(jnp.concatenate([gate_weight, up_weight], axis=1), "z")
    both = across_x(both_z)
    down_z = lax.all_to_all(copies_for(after(down_weight.T, both_z), "z"), "z", 0, 0)
    down = across_x(down_z.reshape(n_z, piece, units))

    widened = tokens.astype(F32)
    scale = lax.rsqrt(jnp.mean(widened * widened, axis=-1, keepdims=True) + epsilon)
    normed = (widened * scale * norm_gain).astype(BF16)
    hidden = local_call(
        hidden_body,
        jax.ShapeDtypeStruct((count, units), BF16),
        [VMEM((n_z, n_x, piece, 2 * units), BF16)],
        1, 5,
    )(x1, normed, *both)
    send, whole = local_call(
        send_body,
        [
            jax.ShapeDtypeStruct((half, width), BF16),
            jax.ShapeDtypeStruct((n_z, n_x, piece, units), BF16),
        ],
        (), 2, 5,
    )(x1, c1, hidden, *down)
    theirs = shift(send, "c", 1)
    keep = local_call(
        keep_body, jax.ShapeDtypeStruct((half, width), BF16), (), 1, 2
    )(c1, hidden, whole)
    pair = local_call(
        pair_sum_body,
        jax.ShapeDtypeStruct(folded, BF16),
        [VMEM((half, width), F32), VMEM(folded, F32)],
        0, 2,
    )(keep, theirs)
    pieces = lax.all_to_all(pair, "y", 0, 0, tiled=True)
    own_tokens = lax.dynamic_slice_in_dim(tokens, c * half + y * rows, rows, 0)
    done = local_call(
        finish_body,
        jax.ShapeDtypeStruct(folded[1:], BF16),
        [VMEM(folded[1:], F32)] * 2,
        0, 3,
    )(pieces, own_tokens, branch_gain[None])
    mine = lax.all_gather(done, "y")
    return local_call(
        join_body,
        jax.ShapeDtypeStruct((count, width), BF16),
        [VMEM((2, *folded), F32), VMEM((2, half, width), F32)],
        1, 2,
    )(c1, mine, shift(mine, "c", 1))


def solution(mesh):
    n_tp = mesh.shape["tp"]
    split = Mesh(mesh.devices.reshape(12, 4, n_tp // 2, 2), ("z", "x", "y", "c"))
    fs, tp = ("z", "x"), ("y", "c")
    placed = (P(fs, None), P(), P(fs, tp), P(fs, tp), P(tp, fs), P())
    return jax.shard_map(
        per_device, mesh=split, in_specs=placed, out_specs=P(fs, None), check_vma=False
    )
```

```python
import jax
import jax.numpy as jnp
from jax import lax
from jax.experimental import pallas as pl
from jax.experimental.pallas import tpu as pltpu
from jax.sharding import Mesh
from jax.sharding import PartitionSpec as P


epsilon = 1e-06
VMEM = pltpu.VMEM
BF16 = jnp.bfloat16
F32 = jnp.float32


def shift(value, axis, by):
    n = lax.axis_size(axis)
    return lax.ppermute(value, axis, [(i, (i + by) % n) for i in range(n)])


def after(value, *others):
    return lax.optimization_barrier((value, *others))[0]


def local_call(body, outs, scratch=(), n_scalars=0, n_in=0, limit=20):
    return pl.pallas_call(
        body,
        out_shape=outs,
        in_specs=[pl.BlockSpec(memory_space=pltpu.SMEM)] * n_scalars
        + [pl.BlockSpec(memory_space=VMEM)] * n_in,
        out_specs=jax.tree.map(lambda _: pl.BlockSpec(memory_space=VMEM), outs),
        scratch_shapes=list(scratch),
        compiler_params=pltpu.CompilerParams(vmem_limit_bytes=limit << 20),
    )


def first_round(block):
    return shift(block, "x", -1), shift(block, "x", 1)


def halves_body(left, right, low, high):
    half = low.shape[0]
    low[...] = left[:half]
    high[...] = right[half:]


def second_round(right, left):
    part = jax.ShapeDtypeStruct((left.shape[0] // 2, *left.shape[1:]), BF16)
    low, high = local_call(halves_body, [part, part], n_in=2, limit=4)(left, right)
    return shift(low, "x", 1), shift(high, "x", -1)


def norm_body(tokens, gain, out):
    step = 16

    def lines(i, carry):
        at = pl.ds(pl.multiple_of(i * step, step), step)
        widened = tokens[at, :].astype(F32)
        scale = lax.rsqrt(jnp.mean(widened * widened, axis=-1, keepdims=True) + epsilon)
        out[at, :] = (widened * scale * gain[...]).astype(BF16)
        return carry

    lax.fori_loop(0, tokens.shape[0] // step, lines, 0)


def interleave(x, own, right, left, low, high, whole):
    slots = [lax.rem(x + k, 4) for k in range(4)]
    half = low.shape[0]
    for z in range(own.shape[0]):
        whole[z, slots[0]] = own[z]
        whole[z, slots[1]] = right[z]
        whole[z, slots[3]] = left[z]
        whole[z, slots[2]] = low[z] if z < half else high[z - half]


def hidden_body(x_ref, normed, own, right, left, low, high, hidden, whole):
    interleave(x_ref[0], own, right, left, low, high, whole)
    planes, across, rows, columns = whole.shape
    weight = whole[...].reshape(planes * across * rows, columns)
    width = columns // 2
    both = jnp.dot(normed[...], weight, preferred_element_type=F32)
    gate, up = both[:, :width], both[:, width:]
    hidden[...] = (gate * jax.nn.sigmoid(gate) * up).astype(BF16)


def half_product(hidden, which, weight):
    half = hidden.shape[0] // 2
    lines = hidden[pl.ds(pl.multiple_of(which * half, 32), half), :]
    planes, across, rows, width = weight.shape
    return lax.dot_general(
        lines,
        weight[...].reshape(planes * across * rows, width),
        (((1,), (1,)), ((), ())),
        preferred_element_type=F32,
    ).astype(BF16)


def send_body(x_ref, c_ref, hidden, own, right, left, low, high, send, whole):
    interleave(x_ref[0], own, right, left, low, high, whole)
    send[...] = half_product(hidden, 1 - c_ref[0], whole)


def keep_body(c_ref, hidden, whole, keep):
    keep[...] = half_product(hidden, c_ref[0], whole)


def pair_sum_body(mine, theirs, out, total, folded):
    total[...] = mine[...].astype(F32) + theirs[...].astype(F32)
    count, rows, width = out.shape
    rows = rows // 2
    for j in range(count):
        for part in range(2):
            folded[j, part * rows : (part + 1) * rows, :] = total[
                j * rows : (j + 1) * rows, part * width : (part + 1) * width
            ]
        out[j] = folded[j].astype(BF16)


def finish_body(pieces, tokens, gain, out, branch, full):
    total = pieces[0].astype(F32)
    for j in range(1, pieces.shape[0]):
        total = total + pieces[j].astype(F32)
    branch[...] = total
    rows, width = tokens.shape[0], total.shape[1]
    parts = [branch[part * rows : (part + 1) * rows, :] for part in range(2)]
    squares = sum(jnp.sum(p * p, axis=-1, keepdims=True) for p in parts)
    scale = lax.rsqrt(squares / (2 * width) + epsilon)
    for part, value in enumerate(parts):
        columns = slice(part * width, (part + 1) * width)
        full[part * rows : (part + 1) * rows, :] = (
            tokens[:, columns].astype(F32) + value * scale * gain[:, columns]
        )
    rounded = full[...].astype(BF16)
    for j in range(out.shape[0]):
        out[j] = rounded


def join_body(c_ref, mine, theirs, out, folded, lines):
    count, rows, width = mine.shape
    rows = rows // 2
    half = count * rows
    for at, (source, which) in enumerate(((mine, c_ref[0]), (theirs, 1 - c_ref[0]))):
        for j in range(count):
            folded[at, j] = source[j].astype(F32)
            for part in range(2):
                lines[at, j * rows : (j + 1) * rows, part * width : (part + 1) * width] = (
                    folded[at, j, part * rows : (part + 1) * rows, :]
                )
        out[pl.ds(pl.multiple_of(which * half, 32), half), :] = lines[at].astype(BF16)


def per_device(tokens, norm_gain, gate_weight, up_weight, down_weight, branch_gain):
    x, y, c = (lax.axis_index(a) for a in ("x", "y", "c"))
    x1, c1 = x.astype(jnp.int32)[None], c.astype(jnp.int32)[None]
    n_x, n_y, n_z = (lax.axis_size(a) for a in ("x", "y", "z"))
    count, width = tokens.shape
    half, rows = count // 2, count // 2 // n_y
    units, piece = gate_weight.shape[1], gate_weight.shape[0]
    folded = (n_y, 2 * rows, width // 2)

    own_tokens = lax.dynamic_slice_in_dim(tokens, c * half + y * rows, rows, 0)
    own_both, own_down, own_tokens, gain, branch_gain = lax.optimization_barrier(
        (
            jnp.concatenate([gate_weight, up_weight], axis=1),
            down_weight.T,
            own_tokens,
            norm_gain[None],
            branch_gain[None],
        )
    )
    both_z = lax.all_gather(own_both, "z")
    near = first_round(both_z)
    down_z = lax.all_gather(after(own_down, both_z), "z")
    far = second_round(*near)
    down_near = first_round(after(down_z, *near))
    down_far = second_round(*down_near)
    normed = local_call(
        norm_body, jax.ShapeDtypeStruct((count, width), BF16), n_in=2, limit=8
    )(tokens, gain)
    hidden = local_call(
        hidden_body,
        jax.ShapeDtypeStruct((count, units), BF16),
        [VMEM((n_z, n_x, piece, 2 * units), BF16)],
        1, 6,
    )(x1, normed, both_z, *near, *far)
    send, whole = local_call(
        send_body,
        [
            jax.ShapeDtypeStruct((half, width), BF16),
            jax.ShapeDtypeStruct((n_z, n_x, piece, units), BF16),
        ],
        (), 2, 6,
    )(x1, c1, hidden, down_z, *down_near, *down_far)
    theirs = shift(send, "c", 1)
    keep = local_call(
        keep_body, jax.ShapeDtypeStruct((half, width), BF16), (), 1, 2
    )(c1, hidden, whole)
    pair = local_call(
        pair_sum_body,
        jax.ShapeDtypeStruct(folded, BF16),
        [VMEM((half, width), F32), VMEM(folded, F32)],
        0, 2,
    )(keep, theirs)
    pieces = lax.all_to_all(pair, "y", 0, 0, tiled=True)
    done = local_call(
        finish_body,
        jax.ShapeDtypeStruct(folded, BF16),
        [VMEM(folded[1:], F32)] * 2,
        0, 3,
    )(pieces, own_tokens, branch_gain)
    mine = lax.all_to_all(done, "y", 0, 0, tiled=True)
    return local_call(
        join_body,
        jax.ShapeDtypeStruct((count, width), BF16),
        [VMEM((2, *folded), F32), VMEM((2, half, width), F32)],
        1, 2,
    )(c1, mine, shift(mine, "c", 1))


def solution(mesh):
    n_tp = mesh.shape["tp"]
    split = Mesh(mesh.devices.reshape(12, 4, n_tp // 2, 2), ("z", "x", "y", "c"))
    fs, tp = ("z", "x"), ("y", "c")
    placed = (P(fs, None), P(), P(fs, tp), P(fs, tp), P(tp, fs), P())

    return jax.shard_map(
        per_device, mesh=split, in_specs=placed, out_specs=P(fs, None), check_vma=False
    )
```

```python
import jax
import jax.numpy as jnp
from jax import lax
from jax.experimental import pallas as pl
from jax.experimental.pallas import tpu as pltpu
from jax.sharding import Mesh
from jax.sharding import PartitionSpec as P


epsilon = 1e-06
VMEM = pltpu.VMEM
BF16 = jnp.bfloat16
F32 = jnp.float32


def shift(value, axis, by):
    n = lax.axis_size(axis)
    return lax.ppermute(value, axis, [(i, (i + by) % n) for i in range(n)])


def after(value, *others):
    return lax.optimization_barrier((value, *others))[0]


def local_call(body, outs, scratch=(), n_scalars=0, n_in=0, limit=20):
    return pl.pallas_call(
        body,
        out_shape=outs,
        in_specs=[pl.BlockSpec(memory_space=pltpu.SMEM)] * n_scalars
        + [pl.BlockSpec(memory_space=VMEM)] * n_in,
        out_specs=jax.tree.map(lambda _: pl.BlockSpec(memory_space=VMEM), outs),
        scratch_shapes=list(scratch),
        compiler_params=pltpu.CompilerParams(vmem_limit_bytes=limit << 20),
    )


def first_round(block):
    return shift(block, "x", -1), shift(block, "x", 1)


def halves_body(left, right, low, high):
    half = low.shape[0]
    low[...] = left[:half]
    high[...] = right[half:]


def second_round(right, left):
    part = jax.ShapeDtypeStruct((left.shape[0] // 2, *left.shape[1:]), BF16)
    low, high = local_call(halves_body, [part, part], n_in=2, limit=4)(left, right)
    return shift(low, "x", 1), shift(high, "x", -1)


def norm_body(tokens, gain, out):
    step = 16

    def lines(i, carry):
        at = pl.ds(pl.multiple_of(i * step, step), step)
        widened = tokens[at, :].astype(F32)
        scale = lax.rsqrt(jnp.mean(widened * widened, axis=-1, keepdims=True) + epsilon)
        out[at, :] = (widened * scale * gain[...]).astype(BF16)
        return carry

    lax.fori_loop(0, tokens.shape[0] // step, lines, 0, unroll=4)


def interleave(x, own, right, left, low, high, whole):
    slots = [lax.rem(x + k, 4) for k in range(4)]
    half = low.shape[0]
    for z in range(own.shape[0]):
        whole[z, slots[0]] = own[z]
        whole[z, slots[1]] = right[z]
        whole[z, slots[3]] = left[z]
        whole[z, slots[2]] = low[z] if z < half else high[z - half]


def hidden_body(x_ref, normed, own, right, left, low, high, hidden, whole):
    interleave(x_ref[0], own, right, left, low, high, whole)
    planes, across, rows, columns = whole.shape
    weight = whole[...].reshape(planes * across * rows, columns)
    width = columns // 2
    both = jnp.dot(normed[...], weight, preferred_element_type=F32)
    gate, up = both[:, :width], both[:, width:]
    hidden[...] = (gate * jax.nn.sigmoid(gate) * up).astype(BF16)


def half_product(hidden, which, weight):
    half = hidden.shape[0] // 2
    lines = hidden[pl.ds(pl.multiple_of(which * half, 32), half), :]
    planes, across, rows, width = weight.shape
    return lax.dot_general(
        lines,
        weight[...].reshape(planes * across * rows, width),
        (((1,), (1,)), ((), ())),
        preferred_element_type=F32,
    ).astype(BF16)


def send_body(x_ref, c_ref, hidden, own, right, left, low, high, send, whole):
    interleave(x_ref[0], own, right, left, low, high, whole)
    send[...] = half_product(hidden, 1 - c_ref[0], whole)


def keep_body(c_ref, hidden, whole, keep):
    keep[...] = half_product(hidden, c_ref[0], whole)


def pair_sum_body(mine, theirs, out, total, folded):
    total[...] = mine[...].astype(F32) + theirs[...].astype(F32)
    count, rows, width = out.shape
    rows = rows // 2
    for j in range(count):
        for part in range(2):
            folded[j, part * rows : (part + 1) * rows, :] = total[
                j * rows : (j + 1) * rows, part * width : (part + 1) * width
            ]
        out[j] = folded[j].astype(BF16)


def finish_body(pieces, tokens, gain, out, branch, full):
    total = pieces[0].astype(F32)
    for j in range(1, pieces.shape[0]):
        total = total + pieces[j].astype(F32)
    branch[...] = total
    rows, width = tokens.shape[0], total.shape[1]
    parts = [branch[part * rows : (part + 1) * rows, :] for part in range(2)]
    squares = sum(jnp.sum(p * p, axis=-1, keepdims=True) for p in parts)
    scale = lax.rsqrt(squares / (2 * width) + epsilon)
    for part, value in enumerate(parts):
        columns = slice(part * width, (part + 1) * width)
        full[part * rows : (part + 1) * rows, :] = (
            tokens[:, columns].astype(F32) + value * scale * gain[:, columns]
        )
    out[...] = full[...].astype(BF16)


def join_body(c_ref, mine, theirs, out, folded, lines):
    count, rows, width = mine.shape
    rows = rows // 2
    half = count * rows
    for at, (source, which) in enumerate(((mine, c_ref[0]), (theirs, 1 - c_ref[0]))):
        for j in range(count):
            folded[at, j] = source[j].astype(F32)
            for part in range(2):
                lines[at, j * rows : (j + 1) * rows, part * width : (part + 1) * width] = (
                    folded[at, j, part * rows : (part + 1) * rows, :]
                )
        out[pl.ds(pl.multiple_of(which * half, 32), half), :] = lines[at].astype(BF16)


def per_device(tokens, norm_gain, gate_weight, up_weight, down_weight, branch_gain):
    x, y, c = (lax.axis_index(a) for a in ("x", "y", "c"))
    x1, c1 = x.astype(jnp.int32)[None], c.astype(jnp.int32)[None]
    n_x, n_y, n_z = (lax.axis_size(a) for a in ("x", "y", "z"))
    count, width = tokens.shape
    half, rows = count // 2, count // 2 // n_y
    units, piece = gate_weight.shape[1], gate_weight.shape[0]
    folded = (n_y, 2 * rows, width // 2)

    both_z = lax.all_gather(jnp.concatenate([gate_weight, up_weight], axis=1), "z")
    near = first_round(both_z)
    copies = jnp.broadcast_to(after(down_weight.T, both_z)[None], (n_z, piece, units))
    down_z = lax.all_to_all(copies, "z", 0, 0, tiled=True)
    normed = local_call(
        norm_body, jax.ShapeDtypeStruct((count, width), BF16), n_in=2, limit=8
    )(tokens, norm_gain[None])
    *near, normed = lax.optimization_barrier((*near, normed))
    far = second_round(*near)
    down_near = first_round(after(down_z, *near))
    hidden = local_call(
        hidden_body,
        jax.ShapeDtypeStruct((count, units), BF16),
        [VMEM((n_z, n_x, piece, 2 * units), BF16)],
        1, 6,
    )(x1, normed, both_z, *near, *far)
    *down_near, hidden = lax.optimization_barrier((*down_near, hidden))
    down_far = second_round(*down_near)
    send, whole = local_call(
        send_body,
        [
            jax.ShapeDtypeStruct((half, width), BF16),
            jax.ShapeDtypeStruct((n_z, n_x, piece, units), BF16),
        ],
        (), 2, 6,
    )(x1, c1, hidden, down_z, *down_near, *down_far)
    theirs = shift(send, "c", 1)
    keep = local_call(
        keep_body, jax.ShapeDtypeStruct((half, width), BF16), (), 1, 2
    )(c1, hidden, whole)
    pair = local_call(
        pair_sum_body,
        jax.ShapeDtypeStruct(folded, BF16),
        [VMEM((half, width), F32), VMEM(folded, F32)],
        0, 2,
    )(keep, theirs)
    pieces = lax.all_to_all(pair, "y", 0, 0, tiled=True)
    own_tokens = lax.dynamic_slice_in_dim(tokens, c * half + y * rows, rows, 0)
    done = local_call(
        finish_body,
        jax.ShapeDtypeStruct(folded[1:], BF16),
        [VMEM(folded[1:], F32)] * 2,
        0, 3,
    )(pieces, own_tokens, branch_gain[None])
    mine = lax.all_gather(done, "y")
    return local_call(
        join_body,
        jax.ShapeDtypeStruct((count, width), BF16),
        [VMEM((2, *folded), F32), VMEM((2, half, width), F32)],
        1, 2,
    )(c1, mine, shift(mine, "c", 1))


def solution(mesh):
    n_tp = mesh.shape["tp"]
    split = Mesh(mesh.devices.reshape(12, 4, n_tp // 2, 2), ("z", "x", "y", "c"))
    fs, tp = ("z", "x"), ("y", "c")
    placed = (P(fs, None), P(), P(fs, tp), P(fs, tp), P(tp, fs), P())

    return jax.shard_map(
        per_device, mesh=split, in_specs=placed, out_specs=P(fs, None), check_vma=False
    )
```

```python
import jax
import jax.numpy as jnp
from jax import lax
from jax.experimental import pallas as pl
from jax.experimental.pallas import tpu as pltpu
from jax.sharding import Mesh
from jax.sharding import PartitionSpec as P


epsilon = 1e-06
VMEM = pltpu.VMEM
BF16 = jnp.bfloat16
F32 = jnp.float32


def shift(value, axis, by):
    n = lax.axis_size(axis)
    return lax.ppermute(value, axis, [(i, (i + by) % n) for i in range(n)])


def after(value, *others):
    return lax.optimization_barrier((value, *others))[0]


def local_call(body, outs, scratch=(), n_scalars=0, n_in=0, limit=20):
    return pl.pallas_call(
        body,
        out_shape=outs,
        in_specs=[pl.BlockSpec(memory_space=pltpu.SMEM)] * n_scalars
        + [pl.BlockSpec(memory_space=VMEM)] * n_in,
        out_specs=jax.tree.map(lambda _: pl.BlockSpec(memory_space=VMEM), outs),
        scratch_shapes=list(scratch),
        compiler_params=pltpu.CompilerParams(vmem_limit_bytes=limit << 20),
    )


def first_round(block):
    return shift(block, "x", -1), shift(block, "x", 1)


def halves_body(left, right, low, high):
    half = low.shape[0]
    low[...] = left[:half]
    high[...] = right[half:]


def second_round(right, left):
    part = jax.ShapeDtypeStruct((left.shape[0] // 2, *left.shape[1:]), BF16)
    low, high = local_call(halves_body, [part, part], n_in=2, limit=4)(left, right)
    return shift(low, "x", 1), shift(high, "x", -1)


def norm_body(c_ref, y_ref, tokens, gain, out, own, window):
    step = 16

    def lines(i, carry):
        at = pl.ds(pl.multiple_of(i * step, step), step)
        widened = tokens[at, :].astype(F32)
        scale = lax.rsqrt(jnp.mean(widened * widened, axis=-1, keepdims=True) + epsilon)
        out[at, :] = (widened * scale * gain[...][None]).astype(BF16)
        return carry

    lax.fori_loop(0, tokens.shape[0] // step, lines, 0, unroll=4)
    count, rows, reach = tokens.shape[0], own.shape[0], window.shape[0]
    first = c_ref[0] * (count // 2) + y_ref[0] * rows
    base = jnp.minimum(first - lax.rem(first, step), count - reach)
    window[...] = tokens[pl.ds(pl.multiple_of(base, step), reach), :].astype(F32)
    for skip in range(0, reach - rows + 1, 4):

        @pl.when(first - base == skip)
        def _():
            own[...] = window[skip : skip + rows, :]


def interleave(x, own, right, left, low, high, whole):
    slots = [lax.rem(x + k, 4) for k in range(4)]
    half = low.shape[0]
    for z in range(own.shape[0]):
        whole[z, slots[0]] = own[z]
        whole[z, slots[1]] = right[z]
        whole[z, slots[3]] = left[z]
        whole[z, slots[2]] = low[z] if z < half else high[z - half]


def hidden_body(x_ref, normed, own, right, left, low, high, hidden, whole):
    interleave(x_ref[0], own, right, left, low, high, whole)
    planes, across, rows, columns = whole.shape
    weight = whole[...].reshape(planes * across * rows, columns)
    width = columns // 2
    both = jnp.dot(normed[...], weight, preferred_element_type=F32)
    gate, up = both[:, :width], both[:, width:]
    hidden[...] = (gate * jax.nn.sigmoid(gate) * up).astype(BF16)


def prepare_body(gate, up, down, both, copies):
    units = gate.shape[1]
    both[:, :units] = gate[...]
    both[:, units:] = up[...]
    for z in range(copies.shape[0]):
        copies[z] = down[...]


def partial_body(x_ref, c_ref, hidden, own, right, left, low, high, send, whole):
    interleave(x_ref[0], own, right, left, low, high, whole)
    send[...] = half_product(hidden, 1 - c_ref[0], whole)


def keep_body(c_ref, hidden, whole, keep):
    keep[...] = half_product(hidden, c_ref[0], whole)


def half_product(hidden, which, whole):
    half = hidden.shape[0] // 2
    lines = hidden[pl.ds(pl.multiple_of(which * half, 32), half), :]
    planes, across, rows, width = whole.shape
    return lax.dot_general(
        lines,
        whole[...].reshape(planes * across * rows, width),
        (((1,), (1,)), ((), ())),
        preferred_element_type=F32,
    ).astype(BF16)


def pair_sum_body(mine, theirs, out, total, folded):
    total[...] = mine[...].astype(F32) + theirs[...].astype(F32)
    count, lines, lanes = out.shape
    parts = total.shape[1] // lanes
    rows = lines // parts
    for j in range(count):
        for t in range(parts):
            folded[j, t * rows : (t + 1) * rows, :] = total[
                j * rows : (j + 1) * rows, t * lanes : (t + 1) * lanes
            ]
        out[j] = folded[j].astype(BF16)


def finish_body(pieces, tokens, gain, out, branch, full):
    count, _, lanes = pieces.shape
    total = pieces[0].astype(F32)
    for j in range(1, count):
        total = total + pieces[j].astype(F32)
    branch[...] = total
    rows, width = tokens.shape
    parts = [branch[t * rows : (t + 1) * rows, :] for t in range(width // lanes)]
    squares = parts[0] * parts[0]
    for value in parts[1:]:
        squares = squares + value * value
    scale = lax.rsqrt(jnp.sum(squares, axis=-1, keepdims=True) / width + epsilon)
    for t, value in enumerate(parts):
        columns = slice(t * lanes, (t + 1) * lanes)
        full[t * rows : (t + 1) * rows, :] = (
            tokens[:, columns] + value * scale * gain[columns][None]
        )
    out[...] = full[...].astype(BF16)


def join_body(c_ref, mine, theirs, out, folded, lines):
    count, _, lanes = mine.shape
    half, width = lines.shape[1:]
    rows = half // count
    for at, (source, which) in enumerate(((mine, c_ref[0]), (theirs, 1 - c_ref[0]))):
        for j in range(count):
            folded[at, j] = source[j].astype(F32)
            for t in range(width // lanes):
                lines[at, j * rows : (j + 1) * rows, t * lanes : (t + 1) * lanes] = (
                    folded[at, j, t * rows : (t + 1) * rows, :]
                )
        out[pl.ds(pl.multiple_of(which * half, 32), half), :] = lines[at].astype(BF16)


def per_device(tokens, norm_gain, gate_weight, up_weight, down_weight, branch_gain):
    places = [lax.axis_index(a).astype(jnp.int32)[None] for a in ("x", "y", "c")]
    gate_weight, x1, y1, c1 = lax.optimization_barrier((gate_weight, *places))
    n_x, n_y, n_z = (lax.axis_size(a) for a in ("x", "y", "z"))
    count, width = tokens.shape
    half, rows = count // 2, count // 2 // n_y
    units, piece = gate_weight.shape[1], gate_weight.shape[0]
    lanes = 128
    flat = (rows * width // lanes, lanes)

    own_both, copies = local_call(
        prepare_body,
        [
            jax.ShapeDtypeStruct((piece, 2 * units), BF16),
            jax.ShapeDtypeStruct((n_z, piece, units), BF16),
        ],
        n_in=3, limit=4,
    )(gate_weight, up_weight, down_weight.T)
    down_z = lax.all_to_all(copies, "z", 0, 0, tiled=True)
    both_z = lax.all_gather(own_both, "z")
    near = first_round(both_z)
    down_near = first_round(after(down_z, both_z))
    normed, own_tokens = local_call(
        norm_body,
        [jax.ShapeDtypeStruct((count, width), BF16), jax.ShapeDtypeStruct((rows, width), F32)],
        [VMEM((48, width), F32)],
        2, 2, 8,
    )(c1, y1, tokens, norm_gain)
    *near, normed = lax.optimization_barrier((*near, normed))
    far = second_round(*near)
    down_far = second_round(*down_near)
    hidden = local_call(
        hidden_body,
        jax.ShapeDtypeStruct((count, units), BF16),
        [VMEM((n_z, n_x, piece, 2 * units), BF16)],
        1, 6,
    )(x1, normed, both_z, *near, *far)

    send, whole = local_call(
        partial_body,
        [
            jax.ShapeDtypeStruct((half, width), BF16),
            jax.ShapeDtypeStruct((n_z, n_x, piece, units), BF16),
        ],
        (), 2, 6,
    )(x1, c1, hidden, down_z, *down_near, *down_far)
    theirs = shift(send, "c", 1)
    keep = local_call(
        keep_body, jax.ShapeDtypeStruct((half, width), BF16), (), 1, 2
    )(c1, hidden, whole)
    folded = (n_y, *flat)
    pair = local_call(
        pair_sum_body,
        jax.ShapeDtypeStruct(folded, BF16),
        [VMEM((half, width), F32), VMEM(folded, F32)],
        0, 2,
    )(keep, theirs)
    pieces = lax.all_to_all(pair, "y", 0, 0, tiled=True)
    done = local_call(
        finish_body,
        jax.ShapeDtypeStruct(flat, BF16),
        [VMEM(flat, F32)] * 2,
        0, 3,
    )(pieces, own_tokens, branch_gain)
    mine = lax.all_gather(done, "y")
    return local_call(
        join_body,
        jax.ShapeDtypeStruct((count, width), BF16),
        [VMEM((2, n_y, *flat), F32), VMEM((2, half, width), F32)],
        1, 2,
    )(c1, mine, shift(mine, "c", 1))


def solution(mesh):
    n_tp = mesh.shape["tp"]
    split = Mesh(mesh.devices.reshape(12, 4, n_tp // 2, 2), ("z", "x", "y", "c"))
    fs, tp = ("z", "x"), ("y", "c")
    placed = (P(fs, None), P(), P(fs, tp), P(fs, tp), P(tp, fs), P())

    return jax.shard_map(
        per_device, mesh=split, in_specs=placed, out_specs=P(fs, None), check_vma=False
    )
```

```python
import jax
import jax.numpy as jnp
from jax import lax
from jax.experimental import pallas as pl
from jax.experimental.pallas import tpu as pltpu
from jax.sharding import Mesh
from jax.sharding import PartitionSpec as P


epsilon = 1e-06
VMEM = pltpu.VMEM
BF16 = jnp.bfloat16
F32 = jnp.float32


def shift(value, axis, by):
    n = lax.axis_size(axis)
    return lax.ppermute(value, axis, [(i, (i + by) % n) for i in range(n)])


def after(value, *others):
    return lax.optimization_barrier((value, *others))[0]


def local_call(body, outs, scratch=(), n_scalars=0, n_in=0, limit=20):
    return pl.pallas_call(
        body,
        out_shape=outs,
        in_specs=[pl.BlockSpec(memory_space=pltpu.SMEM)] * n_scalars
        + [pl.BlockSpec(memory_space=VMEM)] * n_in,
        out_specs=jax.tree.map(lambda _: pl.BlockSpec(memory_space=VMEM), outs),
        scratch_shapes=list(scratch),
        compiler_params=pltpu.CompilerParams(vmem_limit_bytes=limit << 20),
    )


def first_round(block):
    return shift(block, "x", -1), shift(block, "x", 1)


def halves_body(left, right, low, high):
    half = low.shape[0]
    low[...] = left[:half]
    high[...] = right[half:]


def second_round(right, left):
    part = jax.ShapeDtypeStruct((left.shape[0] // 2, *left.shape[1:]), BF16)
    low, high = local_call(halves_body, [part, part], n_in=2, limit=4)(left, right)
    return shift(low, "x", 1), shift(high, "x", -1)


def norm_body(c_ref, y_ref, tokens, gain, out, own, window):
    step = 16

    def lines(i, carry):
        at = pl.ds(pl.multiple_of(i * step, step), step)
        widened = tokens[at, :].astype(F32)
        scale = lax.rsqrt(jnp.mean(widened * widened, axis=-1, keepdims=True) + epsilon)
        out[at, :] = (widened * scale * gain[...][None]).astype(BF16)
        return carry

    lax.fori_loop(0, tokens.shape[0] // step, lines, 0, unroll=4)
    count, rows, reach = tokens.shape[0], own.shape[0], window.shape[0]
    first = c_ref[0] * (count // 2) + y_ref[0] * rows
    base = jnp.minimum(first - lax.rem(first, step), count - reach)
    window[...] = tokens[pl.ds(pl.multiple_of(base, step), reach), :].astype(F32)
    for skip in range(0, reach - rows + 1, 4):

        @pl.when(first - base == skip)
        def _():
            own[...] = window[skip : skip + rows, :]


def interleave(x, own, right, left, low, high, whole):
    slots = [lax.rem(x + k, 4) for k in range(4)]
    half = low.shape[0]
    for z in range(own.shape[0]):
        whole[z, slots[0]] = own[z]
        whole[z, slots[1]] = right[z]
        whole[z, slots[3]] = left[z]
        whole[z, slots[2]] = low[z] if z < half else high[z - half]


def hidden_body(x_ref, normed, own, right, left, low, high, hidden, whole):
    interleave(x_ref[0], own, right, left, low, high, whole)
    planes, across, rows, columns = whole.shape
    weight = whole[...].reshape(planes * across * rows, columns)
    width = columns // 2
    both = jnp.dot(normed[...], weight, preferred_element_type=F32)
    gate, up = both[:, :width], both[:, width:]
    hidden[...] = (gate * jax.nn.sigmoid(gate) * up).astype(BF16)


def copies_body(value, copies):
    for z in range(copies.shape[0]):
        copies[z] = value[...]


def partial_body(x_ref, c_ref, hidden, own, right, left, low, high, send, whole):
    interleave(x_ref[0], own, right, left, low, high, whole)
    send[...] = half_product(hidden, 1 - c_ref[0], whole)


def keep_body(c_ref, hidden, whole, keep):
    keep[...] = half_product(hidden, c_ref[0], whole)


def half_product(hidden, which, whole):
    half = hidden.shape[0] // 2
    lines = hidden[pl.ds(pl.multiple_of(which * half, 32), half), :]
    planes, across, rows, width = whole.shape
    return lax.dot_general(
        lines,
        whole[...].reshape(planes * across * rows, width),
        (((1,), (1,)), ((), ())),
        preferred_element_type=F32,
    ).astype(BF16)


def pair_sum_body(mine, theirs, out, total, folded):
    total[...] = mine[...].astype(F32) + theirs[...].astype(F32)
    count, lines, lanes = out.shape
    parts = total.shape[1] // lanes
    rows = lines // parts
    for j in range(count):
        for t in range(parts):
            folded[j, t * rows : (t + 1) * rows, :] = total[
                j * rows : (j + 1) * rows, t * lanes : (t + 1) * lanes
            ]
        out[j] = folded[j].astype(BF16)


def finish_body(pieces, tokens, gain, out, branch, full):
    count, _, lanes = pieces.shape
    total = pieces[0].astype(F32)
    for j in range(1, count):
        total = total + pieces[j].astype(F32)
    branch[...] = total
    rows, width = tokens.shape
    parts = [branch[t * rows : (t + 1) * rows, :] for t in range(width // lanes)]
    squares = parts[0] * parts[0]
    for value in parts[1:]:
        squares = squares + value * value
    scale = lax.rsqrt(jnp.sum(squares, axis=-1, keepdims=True) / width + epsilon)
    for t, value in enumerate(parts):
        columns = slice(t * lanes, (t + 1) * lanes)
        full[t * rows : (t + 1) * rows, :] = (
            tokens[:, columns] + value * scale * gain[columns][None]
        )
    out[...] = full[...].astype(BF16)


def join_body(c_ref, mine, theirs, out, folded, lines):
    count, _, lanes = mine.shape
    half, width = lines.shape[1:]
    rows = half // count
    for at, (source, which) in enumerate(((mine, c_ref[0]), (theirs, 1 - c_ref[0]))):
        for j in range(count):
            folded[at, j] = source[j].astype(F32)
            for t in range(width // lanes):
                lines[at, j * rows : (j + 1) * rows, t * lanes : (t + 1) * lanes] = (
                    folded[at, j, t * rows : (t + 1) * rows, :]
                )
        out[pl.ds(pl.multiple_of(which * half, 32), half), :] = lines[at].astype(BF16)


def per_device(tokens, norm_gain, gate_weight, up_weight, down_weight, branch_gain):
    places = [lax.axis_index(a).astype(jnp.int32)[None] for a in ("x", "y", "c")]
    gate_weight, x1, y1, c1 = lax.optimization_barrier((gate_weight, *places))
    n_x, n_y, n_z = (lax.axis_size(a) for a in ("x", "y", "z"))
    count, width = tokens.shape
    half, rows = count // 2, count // 2 // n_y
    units, piece = gate_weight.shape[1], gate_weight.shape[0]
    lanes = 128
    flat = (rows * width // lanes, lanes)

    own_both = jnp.concatenate([gate_weight, up_weight], axis=1)
    both_z = lax.all_gather(own_both, "z")
    near = first_round(both_z)
    copies = local_call(
        copies_body, jax.ShapeDtypeStruct((n_z, piece, units), BF16), n_in=1, limit=2
    )(after(down_weight.T, both_z))
    down_z = lax.all_to_all(copies, "z", 0, 0, tiled=True)
    far = second_round(*near)
    down_near = first_round(after(down_z, *near))
    normed, own_tokens = local_call(
        norm_body,
        [jax.ShapeDtypeStruct((count, width), BF16), jax.ShapeDtypeStruct((rows, width), F32)],
        [VMEM((48, width), F32)],
        2, 2, 8,
    )(c1, y1, after(tokens, down_z), norm_gain)
    hidden = local_call(
        hidden_body,
        jax.ShapeDtypeStruct((count, units), BF16),
        [VMEM((n_z, n_x, piece, 2 * units), BF16)],
        1, 6,
    )(x1, normed, both_z, *near, *far)
    *down_near, hidden = lax.optimization_barrier((*down_near, hidden))
    down_far = second_round(*down_near)

    send, whole = local_call(
        partial_body,
        [
            jax.ShapeDtypeStruct((half, width), BF16),
            jax.ShapeDtypeStruct((n_z, n_x, piece, units), BF16),
        ],
        (), 2, 6,
    )(x1, c1, hidden, down_z, *down_near, *down_far)
    theirs = shift(send, "c", 1)
    keep = local_call(
        keep_body, jax.ShapeDtypeStruct((half, width), BF16), (), 1, 2
    )(c1, hidden, whole)
    folded = (n_y, *flat)
    pair = local_call(
        pair_sum_body,
        jax.ShapeDtypeStruct(folded, BF16),
        [VMEM((half, width), F32), VMEM(folded, F32)],
        0, 2,
    )(keep, theirs)
    pieces = lax.all_to_all(pair, "y", 0, 0, tiled=True)
    done = local_call(
        finish_body,
        jax.ShapeDtypeStruct(flat, BF16),
        [VMEM(flat, F32)] * 2,
        0, 3,
    )(pieces, own_tokens, branch_gain)
    mine = lax.all_gather(done, "y")
    return local_call(
        join_body,
        jax.ShapeDtypeStruct((count, width), BF16),
        [VMEM((2, n_y, *flat), F32), VMEM((2, half, width), F32)],
        1, 2,
    )(c1, mine, shift(mine, "c", 1))


def solution(mesh):
    n_tp = mesh.shape["tp"]
    split = Mesh(mesh.devices.reshape(12, 4, n_tp // 2, 2), ("z", "x", "y", "c"))
    fs, tp = ("z", "x"), ("y", "c")
    placed = (P(fs, None), P(), P(fs, tp), P(fs, tp), P(tp, fs), P())

    return jax.shard_map(
        per_device, mesh=split, in_specs=placed, out_specs=P(fs, None), check_vma=False
    )
```

```python
import jax
import jax.numpy as jnp
from jax import lax
from jax.experimental import pallas as pl
from jax.experimental.pallas import tpu as pltpu
from jax.sharding import Mesh
from jax.sharding import PartitionSpec as P


epsilon = 1e-06
VMEM = pltpu.VMEM
BF16 = jnp.bfloat16
F32 = jnp.float32


def shift(value, axis, by):
    n = lax.axis_size(axis)
    return lax.ppermute(value, axis, [(i, (i + by) % n) for i in range(n)])


def after(value, *others):
    return lax.optimization_barrier((value, *others))[0]


def local_call(body, outs, scratch=(), n_scalars=0, n_in=0, limit=20):
    return pl.pallas_call(
        body,
        out_shape=outs,
        in_specs=[pl.BlockSpec(memory_space=pltpu.SMEM)] * n_scalars
        + [pl.BlockSpec(memory_space=VMEM)] * n_in,
        out_specs=jax.tree.map(lambda _: pl.BlockSpec(memory_space=VMEM), outs),
        scratch_shapes=list(scratch),
        compiler_params=pltpu.CompilerParams(vmem_limit_bytes=limit << 20),
    )


def first_round(block):
    return shift(block, "x", -1), shift(block, "x", 1)


def halves_body(left, right, low, high):
    half = low.shape[0]
    low[...] = left[:half]
    high[...] = right[half:]


def second_round(right, left):
    part = jax.ShapeDtypeStruct((left.shape[0] // 2, *left.shape[1:]), BF16)
    low, high = local_call(halves_body, [part, part], n_in=2, limit=4)(left, right)
    return shift(low, "x", 1), shift(high, "x", -1)


def norm_body(c_ref, y_ref, tokens, gain, out, own, window):
    step = 16

    def lines(i, carry):
        at = pl.ds(pl.multiple_of(i * step, step), step)
        widened = tokens[at, :].astype(F32)
        scale = lax.rsqrt(jnp.mean(widened * widened, axis=-1, keepdims=True) + epsilon)
        out[at, :] = (widened * scale * gain[...][None]).astype(BF16)
        return carry

    lax.fori_loop(0, tokens.shape[0] // step, lines, 0, unroll=4)
    count, rows, reach = tokens.shape[0], own.shape[0], window.shape[0]
    first = c_ref[0] * (count // 2) + y_ref[0] * rows
    base = jnp.minimum(first - lax.rem(first, step), count - reach)
    window[...] = tokens[pl.ds(pl.multiple_of(base, step), reach), :].astype(F32)
    for skip in range(0, reach - rows + 1, 4):

        @pl.when(first - base == skip)
        def _():
            own[...] = window[skip : skip + rows, :]


def interleave(x, blocks, whole):
    for offset, block in enumerate(blocks):
        at = lax.rem(x + offset, len(blocks))
        for first, piece in block:
            for z in range(piece.shape[0]):
                whole[first + z, at] = piece[z]


def hidden_body(x_ref, normed, own, right, left, low, high, hidden, whole):
    far = ((0, low), (low.shape[0], high))
    interleave(x_ref[0], (((0, own),), ((0, right),), far, ((0, left),)), whole)
    planes, across, rows, columns = whole.shape
    weight = whole[...].reshape(planes * across * rows, columns)
    width = columns // 2
    both = jnp.dot(normed[...], weight, preferred_element_type=F32)
    gate, up = both[:, :width], both[:, width:]
    hidden[...] = (gate * jax.nn.sigmoid(gate) * up).astype(BF16)


def copies_body(value, copies):
    for z in range(copies.shape[0]):
        copies[z] = value[...]


def partial_body(x_ref, c_ref, hidden, own, right, left, far, send, whole):
    interleave(x_ref[0], [((0, block),) for block in (own, right, far, left)], whole)
    send[...] = half_product(hidden, 1 - c_ref[0], whole)


def keep_body(c_ref, hidden, whole, keep):
    keep[...] = half_product(hidden, c_ref[0], whole)


def half_product(hidden, which, whole):
    half = hidden.shape[0] // 2
    lines = hidden[pl.ds(pl.multiple_of(which * half, 32), half), :]
    planes, across, rows, width = whole.shape
    return lax.dot_general(
        lines,
        whole[...].reshape(planes * across * rows, width),
        (((1,), (1,)), ((), ())),
        preferred_element_type=F32,
    ).astype(BF16)


def pair_sum_body(mine, theirs, out, total, folded):
    total[...] = mine[...].astype(F32) + theirs[...].astype(F32)
    count, lines, lanes = out.shape
    parts = total.shape[1] // lanes
    rows = lines // parts
    for j in range(count):
        for t in range(parts):
            folded[j, t * rows : (t + 1) * rows, :] = total[
                j * rows : (j + 1) * rows, t * lanes : (t + 1) * lanes
            ]
        out[j] = folded[j].astype(BF16)


def finish_body(pieces, tokens, gain, out, branch, full):
    count, _, lanes = pieces.shape
    total = pieces[0].astype(F32)
    for j in range(1, count):
        total = total + pieces[j].astype(F32)
    branch[...] = total
    rows, width = tokens.shape
    parts = [branch[t * rows : (t + 1) * rows, :] for t in range(width // lanes)]
    squares = parts[0] * parts[0]
    for value in parts[1:]:
        squares = squares + value * value
    scale = lax.rsqrt(jnp.sum(squares, axis=-1, keepdims=True) / width + epsilon)
    for t, value in enumerate(parts):
        columns = slice(t * lanes, (t + 1) * lanes)
        full[t * rows : (t + 1) * rows, :] = (
            tokens[:, columns] + value * scale * gain[columns][None]
        )
    out[...] = full[...].astype(BF16)


def join_body(c_ref, mine, theirs, out, folded, lines):
    count, _, lanes = mine.shape
    half, width = lines.shape[1:]
    rows = half // count
    for at, (source, which) in enumerate(((mine, c_ref[0]), (theirs, 1 - c_ref[0]))):
        for j in range(count):
            folded[at, j] = source[j].astype(F32)
            for t in range(width // lanes):
                lines[at, j * rows : (j + 1) * rows, t * lanes : (t + 1) * lanes] = (
                    folded[at, j, t * rows : (t + 1) * rows, :]
                )
        out[pl.ds(pl.multiple_of(which * half, 32), half), :] = lines[at].astype(BF16)


def per_device(tokens, norm_gain, gate_weight, up_weight, down_weight, branch_gain):
    places = [lax.axis_index(a).astype(jnp.int32)[None] for a in ("x", "y", "c")]
    gate_weight, x1, y1, c1 = lax.optimization_barrier((gate_weight, *places))
    n_x, n_y, n_z = (lax.axis_size(a) for a in ("x", "y", "z"))
    count, width = tokens.shape
    half, rows = count // 2, count // 2 // n_y
    units, piece = gate_weight.shape[1], gate_weight.shape[0]
    lanes = 128
    flat = (rows * width // lanes, lanes)

    own_both = jnp.concatenate([gate_weight, up_weight], axis=1)
    both_z = lax.all_gather(own_both, "z")
    near = first_round(both_z)
    copies = local_call(
        copies_body, jax.ShapeDtypeStruct((n_z, piece, units), BF16), n_in=1, limit=2
    )(after(down_weight.T, both_z))
    down_z = lax.all_to_all(copies, "z", 0, 0, tiled=True)
    far = second_round(*near)
    down_z = after(down_z, *near)
    down = (*first_round(down_z), shift(down_z, "x", 2))
    normed, own_tokens = local_call(
        norm_body,
        [jax.ShapeDtypeStruct((count, width), BF16), jax.ShapeDtypeStruct((rows, width), F32)],
        [VMEM((48, width), F32)],
        2, 2, 8,
    )(c1, y1, after(tokens, down_z), norm_gain)
    hidden = local_call(
        hidden_body,
        jax.ShapeDtypeStruct((count, units), BF16),
        [VMEM((n_z, n_x, piece, 2 * units), BF16)],
        1, 6,
    )(x1, normed, both_z, *near, *far)
    send, whole = local_call(
        partial_body,
        [
            jax.ShapeDtypeStruct((half, width), BF16),
            jax.ShapeDtypeStruct((n_z, n_x, piece, units), BF16),
        ],
        (), 2, 5,
    )(x1, c1, hidden, down_z, *down)
    theirs = shift(send, "c", 1)
    keep = local_call(
        keep_body, jax.ShapeDtypeStruct((half, width), BF16), (), 1, 2
    )(c1, hidden, whole)
    folded = (n_y, *flat)
    pair = local_call(
        pair_sum_body,
        jax.ShapeDtypeStruct(folded, BF16),
        [VMEM((half, width), F32), VMEM(folded, F32)],
        0, 2,
    )(keep, theirs)
    pieces = lax.all_to_all(pair, "y", 0, 0, tiled=True)
    done = local_call(
        finish_body,
        jax.ShapeDtypeStruct(flat, BF16),
        [VMEM(flat, F32)] * 2,
        0, 3,
    )(pieces, own_tokens, branch_gain)
    mine = lax.all_gather(done, "y")
    return local_call(
        join_body,
        jax.ShapeDtypeStruct((count, width), BF16),
        [VMEM((2, n_y, *flat), F32), VMEM((2, half, width), F32)],
        1, 2,
    )(c1, mine, shift(mine, "c", 1))


def solution(mesh):
    n_tp = mesh.shape["tp"]
    split = Mesh(mesh.devices.reshape(12, 4, n_tp // 2, 2), ("z", "x", "y", "c"))
    fs, tp = ("z", "x"), ("y", "c")
    placed = (P(fs, None), P(), P(fs, tp), P(fs, tp), P(tp, fs), P())

    return jax.shard_map(
        per_device, mesh=split, in_specs=placed, out_specs=P(fs, None), check_vma=False
    )
```

```python
import jax
import jax.numpy as jnp
from jax import lax
from jax.experimental import pallas as pl
from jax.experimental.pallas import tpu as pltpu
from jax.sharding import Mesh
from jax.sharding import PartitionSpec as P


epsilon = 1e-06
VMEM = pltpu.VMEM
BF16 = jnp.bfloat16
F32 = jnp.float32


def shift(value, axis, by):
    n = lax.axis_size(axis)
    return lax.ppermute(value, axis, [(i, (i + by) % n) for i in range(n)])


def alternating(n):
    return [[2 * y + (h + y) % 2 for y in range(n)] for h in range(2)]


def after(value, *others):
    return lax.optimization_barrier((value, *others))[0]


def local_call(body, outs, scratch=(), n_scalars=0, n_in=0, limit=20):
    return pl.pallas_call(
        body,
        out_shape=outs,
        in_specs=[pl.BlockSpec(memory_space=pltpu.SMEM)] * n_scalars
        + [pl.BlockSpec(memory_space=VMEM)] * n_in,
        out_specs=jax.tree.map(lambda _: pl.BlockSpec(memory_space=VMEM), outs),
        scratch_shapes=list(scratch),
        compiler_params=pltpu.CompilerParams(vmem_limit_bytes=limit << 20),
    )


def first_round(block):
    return shift(block, "x", -1), shift(block, "x", 1)


def halves_body(left, right, low, high):
    half = low.shape[0]
    low[...] = left[:half]
    high[...] = right[half:]


def second_round(right, left):
    part = jax.ShapeDtypeStruct((left.shape[0] // 2, *left.shape[1:]), BF16)
    low, high = local_call(halves_body, [part, part], n_in=2, limit=4)(left, right)
    return shift(low, "x", 1), shift(high, "x", -1)


def norm_body(half_ref, y_ref, tokens, gain, out, own, window):
    step = 16

    def lines(i, carry):
        at = pl.ds(pl.multiple_of(i * step, step), step)
        widened = tokens[at, :].astype(F32)
        scale = lax.rsqrt(jnp.mean(widened * widened, axis=-1, keepdims=True) + epsilon)
        out[at, :] = (widened * scale * gain[...][None]).astype(BF16)
        return carry

    lax.fori_loop(0, tokens.shape[0] // step, lines, 0, unroll=4)
    count, rows, reach = tokens.shape[0], own.shape[0], window.shape[0]
    first = half_ref[0] * (count // 2) + y_ref[0] * rows
    base = jnp.minimum(first - lax.rem(first, step), count - reach)
    window[...] = tokens[pl.ds(pl.multiple_of(base, step), reach), :].astype(F32)
    for skip in range(0, reach - rows + 1, 4):

        @pl.when(first - base == skip)
        def _():
            own[...] = window[skip : skip + rows, :]


def interleave(x, blocks, whole):
    for offset, block in enumerate(blocks):
        at = lax.rem(x + offset, len(blocks))
        for first, piece in block:
            for z in range(piece.shape[0]):
                whole[first + z, at] = piece[z]


def hidden_body(x_ref, normed, own, right, left, low, high, hidden, whole):
    far = ((0, low), (low.shape[0], high))
    interleave(x_ref[0], (((0, own),), ((0, right),), far, ((0, left),)), whole)
    planes, across, rows, columns = whole.shape
    weight = whole[...].reshape(planes * across * rows, columns)
    width = columns // 2
    both = jnp.dot(normed[...], weight, preferred_element_type=F32)
    gate, up = both[:, :width], both[:, width:]
    hidden[...] = (gate * jax.nn.sigmoid(gate) * up).astype(BF16)


def copies_body(value, copies):
    for z in range(copies.shape[0]):
        copies[z] = value[...]


def partial_body(x_ref, half_ref, hidden, own, right, left, far, send, whole):
    interleave(x_ref[0], [((0, block),) for block in (own, right, far, left)], whole)
    send[...] = half_product(hidden, 1 - half_ref[0], whole)


def keep_body(half_ref, hidden, whole, keep):
    keep[...] = half_product(hidden, half_ref[0], whole)


def half_product(hidden, which, whole):
    half = hidden.shape[0] // 2
    lines = hidden[pl.ds(pl.multiple_of(which * half, 32), half), :]
    planes, across, rows, width = whole.shape
    return lax.dot_general(
        lines,
        whole[...].reshape(planes * across * rows, width),
        (((1,), (1,)), ((), ())),
        preferred_element_type=F32,
    ).astype(BF16)


def pair_sum_body(mine, theirs, out, total, folded):
    total[...] = mine[...].astype(F32) + theirs[...].astype(F32)
    count, lines, lanes = out.shape
    parts = total.shape[1] // lanes
    rows = lines // parts
    for j in range(count):
        for t in range(parts):
            folded[j, t * rows : (t + 1) * rows, :] = total[
                j * rows : (j + 1) * rows, t * lanes : (t + 1) * lanes
            ]
        out[j] = folded[j].astype(BF16)


def finish_body(pieces, tokens, gain, out, branch, full):
    count, _, lanes = pieces.shape
    total = pieces[0].astype(F32)
    for j in range(1, count):
        total = total + pieces[j].astype(F32)
    branch[...] = total
    rows, width = tokens.shape
    parts = [branch[t * rows : (t + 1) * rows, :] for t in range(width // lanes)]
    squares = parts[0] * parts[0]
    for value in parts[1:]:
        squares = squares + value * value
    scale = lax.rsqrt(jnp.sum(squares, axis=-1, keepdims=True) / width + epsilon)
    for t, value in enumerate(parts):
        columns = slice(t * lanes, (t + 1) * lanes)
        full[t * rows : (t + 1) * rows, :] = (
            tokens[:, columns] + value * scale * gain[columns][None]
        )
    out[...] = full[...].astype(BF16)


def join_body(which_ref, pieces, *refs):
    out, folded, lines = refs[-3:]
    count, _, lanes = pieces.shape
    half, width = lines.shape
    rows = half // count
    for j in range(count):
        folded[j] = pieces[j].astype(F32)
        for t in range(width // lanes):
            lines[j * rows : (j + 1) * rows, t * lanes : (t + 1) * lanes] = folded[
                j, t * rows : (t + 1) * rows, :
            ]
    out[...] = lines[...].astype(BF16)


def join(which, pieces, half, width, *before):
    grid = pltpu.PrefetchScalarGridSpec(
        num_scalar_prefetch=1,
        grid=(1,),
        in_specs=[pl.BlockSpec(memory_space=VMEM)]
        + [pl.BlockSpec(memory_space=pltpu.HBM)] * len(before),
        out_specs=pl.BlockSpec((half, width), lambda i, which: (which[0], 0)),
        scratch_shapes=[VMEM(pieces.shape, F32), VMEM((half, width), F32)],
    )
    return pl.pallas_call(
        join_body,
        out_shape=jax.ShapeDtypeStruct((2 * half, width), BF16),
        grid_spec=grid,
        input_output_aliases={2: 0} if before else {},
        compiler_params=pltpu.CompilerParams(vmem_limit_bytes=12 << 20),
    )(which, pieces, *before)


def per_device(tokens, norm_gain, gate_weight, up_weight, down_weight, branch_gain):
    x1, y1, c1 = (lax.axis_index(a).astype(jnp.int32)[None] for a in ("x", "y", "c"))
    own_half = lax.rem(c1 + y1, 2)
    gate_weight, x1, y1, own_half, other_half = lax.optimization_barrier(
        (gate_weight, x1, y1, own_half, 1 - own_half)
    )
    n_x, n_y, n_z = (lax.axis_size(a) for a in ("x", "y", "z"))
    count, width = tokens.shape
    half, rows = count // 2, count // 2 // n_y
    units, piece = gate_weight.shape[1], gate_weight.shape[0]
    lanes = 128
    flat = (rows * width // lanes, lanes)

    own_both = jnp.concatenate([gate_weight, up_weight], axis=1)
    both_z = lax.all_gather(own_both, "z")
    near = first_round(both_z)
    copies = local_call(
        copies_body, jax.ShapeDtypeStruct((n_z, piece, units), BF16), n_in=1, limit=2
    )(after(down_weight.T, both_z))
    down_z = lax.all_to_all(copies, "z", 0, 0, tiled=True)
    far = second_round(*near)
    down_z = after(down_z, *near)
    down = (*first_round(down_z), shift(down_z, "x", 2))
    normed, own_tokens = local_call(
        norm_body,
        [jax.ShapeDtypeStruct((count, width), BF16), jax.ShapeDtypeStruct((rows, width), F32)],
        [VMEM((48, width), F32)],
        2, 2, 8,
    )(own_half, y1, after(tokens, down_z), norm_gain)
    hidden = local_call(
        hidden_body,
        jax.ShapeDtypeStruct((count, units), BF16),
        [VMEM((n_z, n_x, piece, 2 * units), BF16)],
        1, 6,
    )(x1, normed, both_z, *near, *far)
    send, whole = local_call(
        partial_body,
        [
            jax.ShapeDtypeStruct((half, width), BF16),
            jax.ShapeDtypeStruct((n_z, n_x, piece, units), BF16),
        ],
        (), 2, 5,
    )(x1, own_half, hidden, down_z, *down)
    theirs = shift(send, "c", 1)
    keep = local_call(
        keep_body, jax.ShapeDtypeStruct((half, width), BF16), (), 1, 2
    )(own_half, hidden, whole)
    folded = (n_y, *flat)
    pair = local_call(
        pair_sum_body,
        jax.ShapeDtypeStruct(folded, BF16),
        [VMEM((half, width), F32), VMEM(folded, F32)],
        0, 2,
    )(keep, theirs)
    pieces = lax.all_to_all(
        pair, ("y", "c"), 0, 0, axis_index_groups=alternating(n_y), tiled=True
    )
    done = local_call(
        finish_body,
        jax.ShapeDtypeStruct(flat, BF16),
        [VMEM(flat, F32)] * 2,
        0, 3,
    )(pieces, own_tokens, branch_gain)
    mine = lax.all_gather(done, ("y", "c"), axis_index_groups=alternating(n_y))
    theirs = shift(mine, "c", 1)
    return join(other_half, theirs, half, width, join(own_half, mine, half, width))


def solution(mesh):
    n_tp = mesh.shape["tp"]
    split = Mesh(mesh.devices.reshape(12, 4, n_tp // 2, 2), ("z", "x", "y", "c"))
    fs, tp = ("z", "x"), ("y", "c")
    placed = (P(fs, None), P(), P(fs, tp), P(fs, tp), P(tp, fs), P())

    return jax.shard_map(
        per_device, mesh=split, in_specs=placed, out_specs=P(fs, None), check_vma=False
    )
```

```python
import jax
import jax.numpy as jnp
from jax import lax
from jax.experimental import pallas as pl
from jax.experimental.pallas import tpu as pltpu
from jax.sharding import Mesh
from jax.sharding import PartitionSpec as P


epsilon = 1e-06
VMEM = pltpu.VMEM
BF16 = jnp.bfloat16
F32 = jnp.float32


def shift(value, axis, by):
    n = lax.axis_size(axis)
    return lax.ppermute(value, axis, [(i, (i + by) % n) for i in range(n)])


def alternating(n):
    return [[2 * y + (h + y) % 2 for y in range(n)] for h in range(2)]


def after(value, *others):
    return lax.optimization_barrier((value, *others))[0]


def local_call(body, outs, scratch=(), n_scalars=0, n_in=0, limit=20):
    return pl.pallas_call(
        body,
        out_shape=outs,
        in_specs=[pl.BlockSpec(memory_space=pltpu.SMEM)] * n_scalars
        + [pl.BlockSpec(memory_space=VMEM)] * n_in,
        out_specs=jax.tree.map(lambda _: pl.BlockSpec(memory_space=VMEM), outs),
        scratch_shapes=list(scratch),
        compiler_params=pltpu.CompilerParams(vmem_limit_bytes=limit << 20),
    )


def first_round(block):
    return shift(block, "x", -1), shift(block, "x", 1)


def halves_body(left, right, low, high):
    half = low.shape[0]
    low[...] = left[:half]
    high[...] = right[half:]


def second_round(right, left):
    part = jax.ShapeDtypeStruct((left.shape[0] // 2, *left.shape[1:]), BF16)
    low, high = local_call(halves_body, [part, part], n_in=2, limit=4)(left, right)
    return shift(low, "x", 1), shift(high, "x", -1)


def norm_body(half_ref, y_ref, tokens, gain, out, own, window):
    step = 16

    def lines(i, carry):
        at = pl.ds(pl.multiple_of(i * step, step), step)
        widened = tokens[at, :].astype(F32)
        scale = lax.rsqrt(jnp.mean(widened * widened, axis=-1, keepdims=True) + epsilon)
        out[at, :] = (widened * scale * gain[...][None]).astype(BF16)
        return carry

    lax.fori_loop(0, tokens.shape[0] // step, lines, 0, unroll=4)
    count, rows, reach = tokens.shape[0], own.shape[0], window.shape[0]
    first = half_ref[0] * (count // 2) + y_ref[0] * rows
    base = jnp.minimum(first - lax.rem(first, step), count - reach)
    window[...] = tokens[pl.ds(pl.multiple_of(base, step), reach), :].astype(F32)
    for skip in range(0, reach - rows + 1, 4):

        @pl.when(first - base == skip)
        def _():
            own[...] = window[skip : skip + rows, :]


def interleave(x, blocks, whole):
    for offset, block in enumerate(blocks):
        at = lax.rem(x + offset, len(blocks))
        for first, piece in block:
            for z in range(piece.shape[0]):
                whole[first + z, at] = piece[z]


def hidden_body(x_ref, normed, own, right, left, low, high, hidden, whole):
    far = ((0, low), (low.shape[0], high))
    interleave(x_ref[0], (((0, own),), ((0, right),), far, ((0, left),)), whole)
    planes, across, rows, columns = whole.shape
    weight = whole[...].reshape(planes * across * rows, columns)
    width = columns // 2
    both = jnp.dot(normed[...], weight, preferred_element_type=F32)
    gate, up = both[:, :width], both[:, width:]
    hidden[...] = (gate * jax.nn.sigmoid(gate) * up).astype(BF16)


def copies_body(value, copies):
    for z in range(copies.shape[0]):
        copies[z] = value[...]


def partial_body(x_ref, half_ref, hidden, own, right, left, far, send, whole):
    interleave(x_ref[0], [((0, block),) for block in (own, right, far, left)], whole)
    send[...] = half_product(hidden, 1 - half_ref[0], whole)


def keep_body(half_ref, hidden, whole, keep):
    keep[...] = half_product(hidden, half_ref[0], whole)


def half_product(hidden, which, whole):
    half = hidden.shape[0] // 2
    lines = hidden[pl.ds(pl.multiple_of(which * half, 32), half), :]
    planes, across, rows, width = whole.shape
    return lax.dot_general(
        lines,
        whole[...].reshape(planes * across * rows, width),
        (((1,), (1,)), ((), ())),
        preferred_element_type=F32,
    ).astype(BF16)


def pair_sum_body(mine, theirs, out):
    out[...] = (mine[...].astype(F32) + theirs[...].astype(F32)).astype(BF16)


def finish_body(summed, tokens, gain, out, folded):
    branch = summed[...].astype(F32)
    scale = lax.rsqrt(jnp.mean(branch * branch, axis=-1, keepdims=True) + epsilon)
    full = tokens[...] + branch * scale * gain[...][None]
    rows, lanes = summed.shape[0], out.shape[1]
    for t in range(summed.shape[1] // lanes):
        folded[t * rows : (t + 1) * rows, :] = full[:, t * lanes : (t + 1) * lanes]
    out[...] = folded[...].astype(BF16)


def join_body(which_ref, pieces, *refs):
    out, folded, lines = refs[-3:]
    count, _, lanes = pieces.shape
    half, width = lines.shape
    rows = half // count
    for j in range(count):
        folded[j] = pieces[j].astype(F32)
        for t in range(width // lanes):
            lines[j * rows : (j + 1) * rows, t * lanes : (t + 1) * lanes] = folded[
                j, t * rows : (t + 1) * rows, :
            ]
    out[...] = lines[...].astype(BF16)


def join(which, pieces, half, width, *before):
    grid = pltpu.PrefetchScalarGridSpec(
        num_scalar_prefetch=1,
        grid=(1,),
        in_specs=[pl.BlockSpec(memory_space=VMEM)]
        + [pl.BlockSpec(memory_space=pltpu.HBM)] * len(before),
        out_specs=pl.BlockSpec((half, width), lambda i, which: (which[0], 0)),
        scratch_shapes=[VMEM(pieces.shape, F32), VMEM((half, width), F32)],
    )
    return pl.pallas_call(
        join_body,
        out_shape=jax.ShapeDtypeStruct((2 * half, width), BF16),
        grid_spec=grid,
        input_output_aliases={2: 0} if before else {},
        compiler_params=pltpu.CompilerParams(vmem_limit_bytes=12 << 20),
    )(which, pieces, *before)


def per_device(tokens, norm_gain, gate_weight, up_weight, down_weight, branch_gain):
    x1, y1, c1 = (lax.axis_index(a).astype(jnp.int32)[None] for a in ("x", "y", "c"))
    own_half = lax.rem(c1 + y1, 2)
    gate_weight, x1, y1, own_half, other_half = lax.optimization_barrier(
        (gate_weight, x1, y1, own_half, 1 - own_half)
    )
    n_x, n_y, n_z = (lax.axis_size(a) for a in ("x", "y", "z"))
    count, width = tokens.shape
    half, rows = count // 2, count // 2 // n_y
    units, piece = gate_weight.shape[1], gate_weight.shape[0]
    lanes = 128
    flat = (rows * width // lanes, lanes)

    own_both = jnp.concatenate([gate_weight, up_weight], axis=1)
    both_z = lax.all_gather(own_both, "z")
    near = first_round(both_z)
    copies = local_call(
        copies_body, jax.ShapeDtypeStruct((n_z, piece, units), BF16), n_in=1, limit=2
    )(after(down_weight.T, both_z))
    down_z = lax.all_to_all(copies, "z", 0, 0, tiled=True)
    far = second_round(*near)
    down_z = after(down_z, *near)
    down = (*first_round(down_z), shift(down_z, "x", 2))
    normed, own_tokens = local_call(
        norm_body,
        [jax.ShapeDtypeStruct((count, width), BF16), jax.ShapeDtypeStruct((rows, width), F32)],
        [VMEM((48, width), F32)],
        2, 2, 8,
    )(own_half, y1, after(tokens, down_z), norm_gain)
    hidden = local_call(
        hidden_body,
        jax.ShapeDtypeStruct((count, units), BF16),
        [VMEM((n_z, n_x, piece, 2 * units), BF16)],
        1, 6,
    )(x1, normed, both_z, *near, *far)
    send, whole = local_call(
        partial_body,
        [
            jax.ShapeDtypeStruct((half, width), BF16),
            jax.ShapeDtypeStruct((n_z, n_x, piece, units), BF16),
        ],
        (), 2, 5,
    )(x1, own_half, hidden, down_z, *down)
    theirs = shift(send, "c", 1)
    keep = local_call(
        keep_body, jax.ShapeDtypeStruct((half, width), BF16), (), 1, 2
    )(own_half, hidden, whole)
    pair = local_call(
        pair_sum_body, jax.ShapeDtypeStruct((half, width), BF16), n_in=2, limit=8
    )(keep, theirs)
    summed = lax.psum_scatter(
        pair,
        ("y", "c"),
        scatter_dimension=0,
        axis_index_groups=alternating(n_y),
        tiled=True,
    )
    done = local_call(
        finish_body, jax.ShapeDtypeStruct(flat, BF16), [VMEM(flat, F32)], n_in=3, limit=8
    )(summed, own_tokens, branch_gain)
    mine = lax.all_gather(done, ("y", "c"), axis_index_groups=alternating(n_y))
    theirs = shift(mine, "c", 1)
    return join(other_half, theirs, half, width, join(own_half, mine, half, width))


def solution(mesh):
    n_tp = mesh.shape["tp"]
    split = Mesh(mesh.devices.reshape(12, 4, n_tp // 2, 2), ("z", "x", "y", "c"))
    fs, tp = ("z", "x"), ("y", "c")
    placed = (P(fs, None), P(), P(fs, tp), P(fs, tp), P(tp, fs), P())

    return jax.shard_map(
        per_device, mesh=split, in_specs=placed, out_specs=P(fs, None), check_vma=False
    )
```

```python
import jax
import jax.numpy as jnp
from jax import lax
from jax.experimental import pallas as pl
from jax.experimental.pallas import tpu as pltpu
from jax.sharding import Mesh
from jax.sharding import PartitionSpec as P


epsilon = 1e-06
VMEM = pltpu.VMEM
BF16 = jnp.bfloat16
F32 = jnp.float32


def shift(value, axis, by):
    n = lax.axis_size(axis)
    return lax.ppermute(value, axis, [(i, (i + by) % n) for i in range(n)])


def alternating(n):
    return [[2 * y + (h + y) % 2 for y in range(n)] for h in range(2)]


def after(value, *others):
    return lax.optimization_barrier((value, *others))[0]


def local_call(body, outs, scratch=(), n_scalars=0, n_in=0, limit=20):
    return pl.pallas_call(
        body,
        out_shape=outs,
        in_specs=[pl.BlockSpec(memory_space=pltpu.SMEM)] * n_scalars
        + [pl.BlockSpec(memory_space=VMEM)] * n_in,
        out_specs=jax.tree.map(lambda _: pl.BlockSpec(memory_space=VMEM), outs),
        scratch_shapes=list(scratch),
        compiler_params=pltpu.CompilerParams(vmem_limit_bytes=limit << 20),
    )


def first_round(block):
    return shift(block, "x", -1), shift(block, "x", 1)


def choose_body(core_ref, right, left, out):
    @pl.when(core_ref[0] == 0)
    def _():
        out[...] = right[...]

    @pl.when(core_ref[0] == 1)
    def _():
        out[...] = left[...]


def second_round(core, right, left):
    onward = local_call(
        choose_body, jax.ShapeDtypeStruct(left.shape, BF16), n_scalars=1, n_in=2, limit=4
    )(core, right, left)
    n = lax.axis_size("x")
    pairs = [(2 * i + k, 2 * ((i + 2 * k - 1) % n) + k) for i in range(n) for k in range(2)]
    return lax.ppermute(onward, ("x", "c"), pairs)


def norm_body(half_ref, y_ref, tokens, gain, out, own, window):
    step = 16

    def lines(i, carry):
        at = pl.ds(pl.multiple_of(i * step, step), step)
        widened = tokens[at, :].astype(F32)
        scale = lax.rsqrt(jnp.mean(widened * widened, axis=-1, keepdims=True) + epsilon)
        out[at, :] = (widened * scale * gain[...][None]).astype(BF16)
        return carry

    lax.fori_loop(0, tokens.shape[0] // step, lines, 0, unroll=4)
    count, rows, reach = tokens.shape[0], own.shape[0], window.shape[0]
    first = half_ref[0] * (count // 2) + y_ref[0] * rows
    base = jnp.minimum(first - lax.rem(first, step), count - reach)
    window[...] = tokens[pl.ds(pl.multiple_of(base, step), reach), :].astype(F32)
    for skip in range(0, reach - rows + 1, 4):

        @pl.when(first - base == skip)
        def _():
            own[...] = window[skip : skip + rows, :]


def interleave(x, blocks, whole):
    for offset, block in enumerate(blocks):
        at = lax.rem(x + offset, len(blocks))
        for z in range(block.shape[0]):
            whole[z, at] = block[z]


def hidden_body(x_ref, normed, own, right, left, far, hidden, whole):
    interleave(x_ref[0], (own, right, far, left), whole)
    planes, across, rows, columns = whole.shape
    weight = whole[...].reshape(planes * across * rows, columns)
    width = columns // 2
    both = jnp.dot(normed[...], weight, preferred_element_type=F32)
    gate, up = both[:, :width], both[:, width:]
    hidden[...] = (gate * jax.nn.sigmoid(gate) * up).astype(BF16)


def copies_body(value, copies):
    for z in range(copies.shape[0]):
        copies[z] = value[...]


def partial_body(x_ref, half_ref, hidden, own, right, left, far, send, whole):
    interleave(x_ref[0], (own, right, far, left), whole)
    send[...] = half_product(hidden, 1 - half_ref[0], whole)


def keep_body(half_ref, hidden, whole, keep):
    keep[...] = half_product(hidden, half_ref[0], whole)


def half_product(hidden, which, whole):
    half = hidden.shape[0] // 2
    lines = hidden[pl.ds(pl.multiple_of(which * half, 32), half), :]
    planes, across, rows, width = whole.shape
    return lax.dot_general(
        lines,
        whole[...].reshape(planes * across * rows, width),
        (((1,), (1,)), ((), ())),
        preferred_element_type=F32,
    ).astype(BF16)


def pair_sum_body(mine, theirs, out):
    out[...] = (mine[...].astype(F32) + theirs[...].astype(F32)).astype(BF16)


def finish_body(summed, tokens, gain, out, folded):
    branch = summed[...].astype(F32)
    scale = lax.rsqrt(jnp.mean(branch * branch, axis=-1, keepdims=True) + epsilon)
    full = tokens[...] + branch * scale * gain[...][None]
    rows, lanes = summed.shape[0], out.shape[1]
    for t in range(summed.shape[1] // lanes):
        folded[t * rows : (t + 1) * rows, :] = full[:, t * lanes : (t + 1) * lanes]
    out[...] = folded[...].astype(BF16)


def join_body(which_ref, pieces, *refs):
    out, folded, lines = refs[-3:]
    count, _, lanes = pieces.shape
    half, width = lines.shape
    rows = half // count
    for j in range(count):
        folded[j] = pieces[j].astype(F32)
        for t in range(width // lanes):
            lines[j * rows : (j + 1) * rows, t * lanes : (t + 1) * lanes] = folded[
                j, t * rows : (t + 1) * rows, :
            ]
    out[...] = lines[...].astype(BF16)


def join(which, pieces, half, width, *before):
    grid = pltpu.PrefetchScalarGridSpec(
        num_scalar_prefetch=1,
        grid=(1,),
        in_specs=[pl.BlockSpec(memory_space=VMEM)]
        + [pl.BlockSpec(memory_space=pltpu.HBM)] * len(before),
        out_specs=pl.BlockSpec((half, width), lambda i, which: (which[0], 0)),
        scratch_shapes=[VMEM(pieces.shape, F32), VMEM((half, width), F32)],
    )
    return pl.pallas_call(
        join_body,
        out_shape=jax.ShapeDtypeStruct((2 * half, width), BF16),
        grid_spec=grid,
        input_output_aliases={2: 0} if before else {},
        compiler_params=pltpu.CompilerParams(vmem_limit_bytes=12 << 20),
    )(which, pieces, *before)


def per_device(tokens, norm_gain, gate_weight, up_weight, down_weight, branch_gain):
    x1, y1, c1 = (lax.axis_index(a).astype(jnp.int32)[None] for a in ("x", "y", "c"))
    own_half = lax.rem(c1 + y1, 2)
    gate_weight, x1, y1, c1, own_half, other_half = lax.optimization_barrier(
        (gate_weight, x1, y1, c1, own_half, 1 - own_half)
    )
    n_x, n_y, n_z = (lax.axis_size(a) for a in ("x", "y", "z"))
    count, width = tokens.shape
    half, rows = count // 2, count // 2 // n_y
    units, piece = gate_weight.shape[1], gate_weight.shape[0]
    lanes = 128
    flat = (rows * width // lanes, lanes)

    own_both = jnp.concatenate([gate_weight, up_weight], axis=1)
    both_z = lax.all_gather(own_both, "z")
    near = first_round(both_z)
    copies = local_call(
        copies_body, jax.ShapeDtypeStruct((n_z, piece, units), BF16), n_in=1, limit=2
    )(after(down_weight.T, both_z))
    down_z = lax.all_to_all(copies, "z", 0, 0, tiled=True)
    far = second_round(c1, *near)
    down_z = after(down_z, *near)
    down_near = first_round(down_z)
    normed, own_tokens = local_call(
        norm_body,
        [jax.ShapeDtypeStruct((count, width), BF16), jax.ShapeDtypeStruct((rows, width), F32)],
        [VMEM((48, width), F32)],
        2, 2, 8,
    )(own_half, y1, after(tokens, down_z), norm_gain)
    *down_near, normed = lax.optimization_barrier((*down_near, normed))
    hidden = local_call(
        hidden_body,
        jax.ShapeDtypeStruct((count, units), BF16),
        [VMEM((n_z, n_x, piece, 2 * units), BF16)],
        1, 5,
    )(x1, normed, both_z, *near, far)
    down = (*down_near, second_round(c1, *down_near))
    send, whole = local_call(
        partial_body,
        [
            jax.ShapeDtypeStruct((half, width), BF16),
            jax.ShapeDtypeStruct((n_z, n_x, piece, units), BF16),
        ],
        (), 2, 5,
    )(x1, own_half, hidden, down_z, *down)
    theirs = shift(send, "c", 1)
    keep = local_call(
        keep_body, jax.ShapeDtypeStruct((half, width), BF16), (), 1, 2
    )(own_half, hidden, whole)
    pair = local_call(
        pair_sum_body, jax.ShapeDtypeStruct((half, width), BF16), n_in=2, limit=8
    )(keep, theirs)
    summed = lax.psum_scatter(
        pair,
        ("y", "c"),
        scatter_dimension=0,
        axis_index_groups=alternating(n_y),
        tiled=True,
    )
    done = local_call(
        finish_body, jax.ShapeDtypeStruct(flat, BF16), [VMEM(flat, F32)], n_in=3, limit=8
    )(summed, own_tokens, branch_gain)
    mine = lax.all_gather(done, ("y", "c"), axis_index_groups=alternating(n_y))
    theirs = shift(mine, "c", 1)
    return join(other_half, theirs, half, width, join(own_half, mine, half, width))


def solution(mesh):
    n_tp = mesh.shape["tp"]
    split = Mesh(mesh.devices.reshape(12, 4, n_tp // 2, 2), ("z", "x", "y", "c"))
    fs, tp = ("z", "x"), ("y", "c")
    placed = (P(fs, None), P(), P(fs, tp), P(fs, tp), P(tp, fs), P())

    return jax.shard_map(
        per_device, mesh=split, in_specs=placed, out_specs=P(fs, None), check_vma=False
    )
```

```python
import functools

import jax
import jax.numpy as jnp
from jax import lax
from jax.experimental import pallas as pl
from jax.experimental.pallas import tpu as pltpu
from jax.sharding import Mesh
from jax.sharding import PartitionSpec as P


epsilon = 1e-06
VMEM = pltpu.VMEM
BF16 = jnp.bfloat16
F32 = jnp.float32


def shift(value, axis, by):
    n = lax.axis_size(axis)
    return lax.ppermute(value, axis, [(i, (i + by) % n) for i in range(n)])


def alternating(n):
    return [[2 * y + (h + y) % 2 for y in range(n)] for h in range(2)]


def after(value, *others):
    return lax.optimization_barrier((value, *others))[0]


def local_call(body, outs, scratch=(), n_scalars=0, n_in=0, limit=20):
    return pl.pallas_call(
        body,
        out_shape=outs,
        in_specs=[pl.BlockSpec(memory_space=pltpu.SMEM)] * n_scalars
        + [pl.BlockSpec(memory_space=VMEM)] * n_in,
        out_specs=jax.tree.map(lambda _: pl.BlockSpec(memory_space=VMEM), outs),
        scratch_shapes=list(scratch),
        compiler_params=pltpu.CompilerParams(vmem_limit_bytes=limit << 20),
    )


def first_round(block):
    return shift(block, "x", -1), shift(block, "x", 1)


def halves_body(left, right, low, high):
    half = low.shape[0]
    low[...] = left[:half]
    high[...] = right[half:]


def second_round(right, left):
    part = jax.ShapeDtypeStruct((left.shape[0] // 2, *left.shape[1:]), BF16)
    low, high = local_call(halves_body, [part, part], n_in=2, limit=4)(left, right)
    return shift(low, "x", 1), shift(high, "x", -1)


def norm_body(half_ref, y_ref, tokens, gain, out, own, window):
    step = 16

    def lines(i, carry):
        at = pl.ds(pl.multiple_of(i * step, step), step)
        widened = tokens[at, :].astype(F32)
        scale = lax.rsqrt(jnp.mean(widened * widened, axis=-1, keepdims=True) + epsilon)
        out[at, :] = (widened * scale * gain[...][None]).astype(BF16)
        return carry

    lax.fori_loop(0, tokens.shape[0] // step, lines, 0, unroll=4)
    count, rows, reach = tokens.shape[0], own.shape[0], window.shape[0]
    first = half_ref[0] * (count // 2) + y_ref[0] * rows
    base = jnp.minimum(first - lax.rem(first, step), count - reach)
    window[...] = tokens[pl.ds(pl.multiple_of(base, step), reach), :].astype(F32)
    for skip in range(0, reach - rows + 1, 4):

        @pl.when(first - base == skip)
        def _():
            own[...] = window[skip : skip + rows, :]


def interleave(x, blocks, whole):
    for offset, block in enumerate(blocks):
        at = lax.rem(x + offset, len(blocks))
        for first, piece in block:
            for z in range(piece.shape[0]):
                whole[first + z, at] = piece[z]


def hidden_body(x_ref, normed, own, right, left, low, high, hidden, whole):
    far = ((0, low), (low.shape[0], high))
    interleave(x_ref[0], (((0, own),), ((0, right),), far, ((0, left),)), whole)
    planes, across, rows, columns = whole.shape
    weight = whole[...].reshape(planes * across * rows, columns)
    width = columns // 2
    both = jnp.dot(normed[...], weight, preferred_element_type=F32)
    gate, up = both[:, :width], both[:, width:]
    hidden[...] = (gate * jax.nn.sigmoid(gate) * up).astype(BF16)


def copies_body(value, copies):
    for z in range(copies.shape[0]):
        copies[z] = value[...]


def partial_body(x_ref, half_ref, hidden, own, right, left, far, send, whole):
    interleave(x_ref[0], [((0, block),) for block in (own, right, far, left)], whole)
    send[...] = half_product(hidden, 1 - half_ref[0], whole)


def keep_body(half_ref, hidden, whole, keep):
    keep[...] = half_product(hidden, half_ref[0], whole)


def half_product(hidden, which, whole):
    half = hidden.shape[0] // 2
    lines = hidden[pl.ds(pl.multiple_of(which * half, 32), half), :]
    planes, across, rows, width = whole.shape
    return lax.dot_general(
        lines,
        whole[...].reshape(planes * across * rows, width),
        (((1,), (1,)), ((), ())),
        preferred_element_type=F32,
    ).astype(BF16)


def pair_sum_body(keepers, mine, theirs, out, total, folded):
    total[...] = mine[...].astype(F32) + theirs[...].astype(F32)
    pieces = total.shape[1] // out.shape[1]
    wide, rows = out.shape[1], total.shape[0] // keepers
    for j in range(keepers):
        for t in range(pieces):
            at = (j * pieces + t) * rows
            folded[at : at + rows, :] = total[
                j * rows : (j + 1) * rows, t * wide : (t + 1) * wide
            ]
    out[...] = folded[...].astype(BF16)


def finish_body(summed, tokens, gain, out, branch, folded):
    branch[...] = summed[...].astype(F32)
    rows, width = tokens.shape
    wide, lanes = summed.shape[1], out.shape[1]
    parts = [branch[t * rows : (t + 1) * rows, :] for t in range(width // wide)]
    squares = parts[0] * parts[0]
    for value in parts[1:]:
        squares = squares + value * value
    scale = lax.rsqrt(jnp.sum(squares, axis=-1, keepdims=True) / width + epsilon)
    for t, value in enumerate(parts):
        columns = slice(t * wide, (t + 1) * wide)
        full = tokens[:, columns] + value * scale * gain[columns][None]
        for u in range(wide // lanes):
            at = (t * (wide // lanes) + u) * rows
            folded[at : at + rows, :] = full[:, u * lanes : (u + 1) * lanes]
    out[...] = folded[...].astype(BF16)


def join_body(which_ref, pieces, *refs):
    out, folded, lines = refs[-3:]
    count, _, lanes = pieces.shape
    half, width = lines.shape
    rows = half // count
    for j in range(count):
        folded[j] = pieces[j].astype(F32)
        for t in range(width // lanes):
            lines[j * rows : (j + 1) * rows, t * lanes : (t + 1) * lanes] = folded[
                j, t * rows : (t + 1) * rows, :
            ]
    out[...] = lines[...].astype(BF16)


def join(which, pieces, half, width, *before):
    grid = pltpu.PrefetchScalarGridSpec(
        num_scalar_prefetch=1,
        grid=(1,),
        in_specs=[pl.BlockSpec(memory_space=VMEM)]
        + [pl.BlockSpec(memory_space=pltpu.HBM)] * len(before),
        out_specs=pl.BlockSpec((half, width), lambda i, which: (which[0], 0)),
        scratch_shapes=[VMEM(pieces.shape, F32), VMEM((half, width), F32)],
    )
    return pl.pallas_call(
        join_body,
        out_shape=jax.ShapeDtypeStruct((2 * half, width), BF16),
        grid_spec=grid,
        input_output_aliases={2: 0} if before else {},
        compiler_params=pltpu.CompilerParams(vmem_limit_bytes=12 << 20),
    )(which, pieces, *before)


def per_device(tokens, norm_gain, gate_weight, up_weight, down_weight, branch_gain):
    x1, y1, c1 = (lax.axis_index(a).astype(jnp.int32)[None] for a in ("x", "y", "c"))
    own_half = lax.rem(c1 + y1, 2)
    gate_weight, x1, y1, own_half, other_half = lax.optimization_barrier(
        (gate_weight, x1, y1, own_half, 1 - own_half)
    )
    n_x, n_y, n_z = (lax.axis_size(a) for a in ("x", "y", "z"))
    count, width = tokens.shape
    half, rows = count // 2, count // 2 // n_y
    units, piece = gate_weight.shape[1], gate_weight.shape[0]
    lanes = 128
    flat = (rows * width // lanes, lanes)

    own_both = jnp.concatenate([gate_weight, up_weight], axis=1)
    both_z = lax.all_gather(own_both, "z")
    near = first_round(both_z)
    copies = local_call(
        copies_body, jax.ShapeDtypeStruct((n_z, piece, units), BF16), n_in=1, limit=2
    )(after(down_weight.T, both_z))
    down_z = lax.all_to_all(copies, "z", 0, 0, tiled=True)
    far = second_round(*near)
    down_z = after(down_z, *near)
    down_far = shift(down_z, "x", 2)
    down = (*first_round(down_z), down_far)
    normed, own_tokens = local_call(
        norm_body,
        [jax.ShapeDtypeStruct((count, width), BF16), jax.ShapeDtypeStruct((rows, width), F32)],
        [VMEM((48, width), F32)],
        2, 2, 8,
    )(own_half, y1, after(tokens, down_z), norm_gain)
    hidden = local_call(
        hidden_body,
        jax.ShapeDtypeStruct((count, units), BF16),
        [VMEM((n_z, n_x, piece, 2 * units), BF16)],
        1, 6,
    )(x1, normed, both_z, *near, *far)
    send, whole = local_call(
        partial_body,
        [
            jax.ShapeDtypeStruct((half, width), BF16),
            jax.ShapeDtypeStruct((n_z, n_x, piece, units), BF16),
        ],
        (), 2, 5,
    )(x1, own_half, hidden, down_z, *down)
    theirs = shift(send, "c", 1)
    keep = local_call(
        keep_body, jax.ShapeDtypeStruct((half, width), BF16), (), 1, 2
    )(own_half, hidden, whole)
    wide = 256
    stacked = (half * width // wide, wide)
    pair = local_call(
        functools.partial(pair_sum_body, n_y),
        jax.ShapeDtypeStruct(stacked, BF16),
        [VMEM((half, width), F32), VMEM(stacked, F32)],
        0, 2, 12,
    )(keep, theirs)
    summed = lax.psum_scatter(
        pair,
        ("y", "c"),
        scatter_dimension=0,
        axis_index_groups=alternating(n_y),
        tiled=True,
    )
    done = local_call(
        finish_body,
        jax.ShapeDtypeStruct(flat, BF16),
        [VMEM((rows * width // wide, wide), F32), VMEM(flat, F32)],
        0, 3, 8,
    )(summed, own_tokens, branch_gain)
    mine = lax.all_gather(done, ("y", "c"), axis_index_groups=alternating(n_y))
    theirs = shift(mine, "c", 1)
    return join(other_half, theirs, half, width, join(own_half, mine, half, width))


def solution(mesh):
    n_tp = mesh.shape["tp"]
    split = Mesh(mesh.devices.reshape(12, 4, n_tp // 2, 2), ("z", "x", "y", "c"))
    fs, tp = ("z", "x"), ("y", "c")
    placed = (P(fs, None), P(), P(fs, tp), P(fs, tp), P(tp, fs), P())

    return jax.shard_map(
        per_device, mesh=split, in_specs=placed, out_specs=P(fs, None), check_vma=False
    )
```
